512 devices in a mesh: sp: 32 (over z, core), tp: 16 (over y, x).
Axes of the slice: x: 4, y: 4, z: 16, core: 2. Of those that a mesh axis runs over, the one named last changes fastest.
Arguments:
- wide_queries: bfloat16 [2048, 2560], P('sp', 'tp'), may hold values from -512 to 512
- narrow_queries: bfloat16 [2048, 1536], P('sp', 'tp'), may hold values from -512 to 512
- kv_latent: bfloat16 [2048, 512], P('sp'), may hold values from -6 to 6
- rope_key: bfloat16 [2048, 32], P('sp'), may hold values from -4 to 4
- latent_gain: float32 [512], replicated, may hold values from 0.1 to 1.9
- wide_kv_weight: bfloat16 [512, 4096], P(None, 'tp'), may hold values from -0.25 to 0.25
- narrow_kv_weight: bfloat16 [512, 2048], P(None, 'tp'), may hold values from -0.25 to 0.25
- wide_out_weight: bfloat16 [2048, 2048], P('tp'), may hold values from -0.4375 to 0.4375
- narrow_out_weight: bfloat16 [1024, 2048], P('tp'), may hold values from -0.4375 to 0.4375
- residual: bfloat16 [2048, 2048], P('sp'), may hold values from -6 to 6
- norm_gain: float32 [2048], replicated, may hold values from 0.1 to 1.9
- route_ids: int32 [2048, 2], P('sp'), may hold values from 0 to 63, all different within a row; in each aligned block of 64 rows (0 to 63, 64 to 127, ...) at most 3 rows name the same one
- route_weights: float32 [2048, 2], P('sp'), may hold values from 0.3 to 1.3
- expert_gate: bfloat16 [64, 2048, 1024], P('sp', None, 'tp'), may hold values from -0.125 to 0.125
- expert_up: bfloat16 [64, 2048, 1024], P('sp', None, 'tp'), may hold values from -0.125 to 0.125
- expert_down: bfloat16 [64, 1024, 2048], P('sp', 'tp'), may hold values from -0.1875 to 0.1875
- shared_gate: bfloat16 [2048, 1024], P(None, 'tp'), may hold values from -0.125 to 0.125
- shared_up: bfloat16 [2048, 1024], P(None, 'tp'), may hold values from -0.125 to 0.125
- shared_down: bfloat16 [1024, 2048], P('tp'), may hold values from -0.1875 to 0.1875
Outputs:
- mixed_out: bfloat16 [2048, 2048], P('sp', 'tp')
The draws below stay inside these ranges and needn't reach their ends.
Inputs may be any that keep to these rules, and one draw needn't show every extreme that they name: `route_ids`: in the rows of one index of sp (aligned blocks of 64 rows) no expert is named by more than 3 rows, and some expert by exactly that many; each row names 2 different experts.
All inputs are finite; a program needn't handle non-finite values.
Results may differ from the reference program's by a relative error of at most 0.018.
Values may be sent and summed in bfloat16 or wider, within the bound.
No kernel may reach another device: no remote copies, remote signals or barrier semaphores. Data moves between devices by JAX's collectives and lax.ppermute only.
A program may use at most 64 MiB of HBM per device.

```python
import math
import jax
import jax.numpy as jnp
import numpy as np
from jax import lax

D_MODEL = 2048
WIDE_HEADS = 16
NARROW_HEADS = 16
WIDE_NOPE = 128
WIDE_VALUE = 128
NARROW_NOPE = 64
NARROW_VALUE = 64
ROPE_DIM = 32
LATENT = 512
EXPERT_FF = 1024
TOP_K = 2
TOK_DEV = 64
TOKENS = 2048
EXPERTS = 64
CAPACITY = 3
N_SP = 32
N_TP = 16


def queries_for(key, head_count, nope_width, salt):
    full_width = nope_width + ROPE_DIM
    base = 2.0 * jax.random.normal(jax.random.fold_in(key, salt), (TOKENS, head_count, full_width), jnp.float32)
    base = jnp.clip(base, -12.0, 12.0)
    return base.reshape(TOKENS, head_count * full_width).astype(jnp.bfloat16)


def draw_wide_queries(key, part):
    return queries_for(key, WIDE_HEADS, WIDE_NOPE, 31)


def draw_narrow_queries(key, part):
    return queries_for(key, NARROW_HEADS, NARROW_NOPE, 32)


def draw_rope_key(key, part):
    base = jnp.clip(jax.random.normal(jax.random.fold_in(key, 21), (TOKENS, ROPE_DIM), jnp.float32), -4.0, 4.0)
    return base.astype(jnp.bfloat16)


def shard_levels(rng, shape, split, least, top_value):
    loudness, own = 1.0, jax.random.fold_in(rng, 6)
    for axis_at, blocks in split:
        draws = jnp.exp(jax.random.uniform(jax.random.fold_in(own, axis_at), (blocks,), jnp.float32, least / len(split), top_value / len(split)))
        loudness = loudness * jnp.repeat(draws, shape[axis_at] // blocks).reshape([-1 if axis == axis_at else 1 for axis in range(len(shape))])
    return loudness


def routed_block(own_key, own, number, rows, count, top, most, lean):
    ranking = jax.random.permutation(own_key, count)
    packed, usual = portions_of(count, rows * top, most, lean, True), portions_of(count, rows * top, most, lean, False)
    places = jnp.arange(count)

    def named(lengths, turn):
        used = int((lengths > 0).sum())
        fixed = max(1, used // 4)
        moved = fixed + (places - fixed + turn * (used - fixed)) % max(1, count - fixed)
        return jnp.zeros((count,), jnp.int32).at[ranking[jnp.where(places < fixed, places, moved)]].set(jnp.asarray(lengths, jnp.int32))

    lengths = jnp.where(number % 4 == 0, named(packed, number // 4), named(usual, number - number // 4 - 1))
    mixed = jax.random.permutation(jax.random.fold_in(own, 3), count)
    source_of, sink = mixed[0:count // 2 * 2:2], mixed[1:count // 2 * 2:2]
    room = jnp.minimum(lengths[source_of] - 1, most - lengths[sink]) // 2
    room = jnp.where((source_of == ranking[0]) | (sink == ranking[0]) | (lengths[sink] == 0), 0, jnp.maximum(room, 0))
    moved = jax.random.randint(jax.random.fold_in(own, 4), (count // 2,), 0, 1 << 20) % (room + 1)
    lengths = lengths.at[source_of].add(-moved).at[sink].add(moved)
    members = jnp.searchsorted(jnp.cumsum(lengths), jnp.arange(rows * top), side="right").astype(jnp.int32)
    table = members.reshape(top, rows).T
    table = table[jax.random.permutation(jax.random.fold_in(own, 1), rows)]
    turn = jax.random.randint(jax.random.fold_in(own, 2), (rows, 1), 0, top)
    return jnp.take_along_axis(table, (jnp.arange(top)[None, :] + turn) % top, axis=1)


def portions_of(count, total, reach, lean, full):
    portions = [(1 << 20) // math.isqrt(rank ** lean) + 1 for rank in range(1, count + 1)]
    largest = reach if full else min(reach, max(-(-total // count), total * portions[0] // sum(portions)))
    least = 1 if total - largest >= count - 1 else 0
    given, rest = [largest] + [least] * (count - 1), total - largest - least * (count - 1)
    while rest > 0:
        free = [i for i in range(1, count) if given[i] < largest] or [i for i in range(1, count) if given[i] < reach]
        mass, remaining = sum([portions[i] for i in free]), rest
        for i in free:
            addition = min(reach - given[i], max(1, remaining * portions[i] // mass), rest)
            given[i] = given[i] + addition
            rest = rest - addition
    return np.array(given)


def normal_values(rng, dims, scale, reach, split=(), kind=jnp.bfloat16):
    entries = scale * jax.random.normal(rng, dims, jnp.float32)
    if split:
        entries = entries * shard_levels(rng, dims, split, -0.22, 0.18)
    return jnp.clip(entries, -reach, reach).astype(kind)


def setup_inputs(seed: int = 0) -> dict:
    key_list = jax.random.split(jax.random.key(seed), 20)
    wide_queries = draw_wide_queries(jax.random.fold_in(key_list[19], 71), 0)
    narrow_queries = draw_narrow_queries(jax.random.fold_in(key_list[19], 71), 0)
    kv_latent = normal_values(key_list[2], (TOKENS, LATENT), 1.0, 6.0, ((0, 32),))
    rope_key = draw_rope_key(jax.random.fold_in(key_list[19], 71), 0)
    latent_gain = jnp.clip(1.0 + 0.18 * jax.random.normal(key_list[4], (LATENT,), jnp.float32), 0.1, 1.9)
    wide_kv_weight = normal_values(key_list[5], (LATENT, WIDE_HEADS * (WIDE_NOPE + WIDE_VALUE)), LATENT ** -0.5, 0.25, ((1, 16),))
    narrow_kv_weight = normal_values(key_list[6], (LATENT, NARROW_HEADS * (NARROW_NOPE + NARROW_VALUE)), LATENT ** -0.5, 0.25, ((1, 16),))
    wide_out_weight = normal_values(key_list[7], (WIDE_HEADS * WIDE_VALUE, D_MODEL), ((WIDE_HEADS * WIDE_VALUE + NARROW_HEADS * NARROW_VALUE) // 16) ** -0.5, 0.4375, ((0, 16),))
    narrow_out_weight = normal_values(key_list[8], (NARROW_HEADS * NARROW_VALUE, D_MODEL), ((WIDE_HEADS * WIDE_VALUE + NARROW_HEADS * NARROW_VALUE) // 16) ** -0.5, 0.4375, ((0, 16),))
    residual = normal_values(key_list[9], (TOKENS, D_MODEL), 1.0, 6.0, ((0, 32),))
    norm_gain = jnp.clip(1.0 + 0.18 * jax.random.normal(key_list[10], (D_MODEL,), jnp.float32), 0.1, 1.9)
    route_ids_keys = jax.random.split(jax.random.fold_in(key_list[11], 1), TOKENS // TOK_DEV)
    route_ids_turns = jax.random.permutation(jax.random.fold_in(key_list[11], 3), TOKENS // TOK_DEV)
    route_ids = jax.vmap(lambda own, number: routed_block(jax.random.fold_in(key_list[11], 2), own, number, TOK_DEV, EXPERTS, TOP_K, CAPACITY, 1))(route_ids_keys, route_ids_turns).reshape((TOKENS, TOP_K))
    route_weights = jnp.clip(0.3 + 0.99999994 * jax.random.uniform(key_list[12], (TOKENS, TOP_K), jnp.float32) ** shard_levels(key_list[12], (TOKENS, TOP_K), ((0, 32),), -0.2, 0.2), 0.3, 1.3)
    expert_gate = normal_values(key_list[13], (EXPERTS, D_MODEL, EXPERT_FF), D_MODEL ** -0.5, 0.125, ((0, 32), (2, 16)))
    expert_up = normal_values(key_list[14], (EXPERTS, D_MODEL, EXPERT_FF), D_MODEL ** -0.5, 0.125, ((0, 32), (2, 16)))
    expert_down = normal_values(key_list[15], (EXPERTS, EXPERT_FF, D_MODEL), EXPERT_FF ** -0.5, 0.1875, ((0, 32), (1, 16)))
    shared_gate = normal_values(key_list[16], (D_MODEL, EXPERT_FF), D_MODEL ** -0.5, 0.125, ((1, 16),))
    shared_up = normal_values(key_list[17], (D_MODEL, EXPERT_FF), D_MODEL ** -0.5, 0.125, ((1, 16),))
    shared_down = normal_values(key_list[18], (EXPERT_FF, D_MODEL), EXPERT_FF ** -0.5, 0.1875, ((0, 16),))
    return dict(wide_queries=wide_queries, narrow_queries=narrow_queries, kv_latent=kv_latent, rope_key=rope_key, latent_gain=latent_gain, wide_kv_weight=wide_kv_weight, narrow_kv_weight=narrow_kv_weight, wide_out_weight=wide_out_weight, narrow_out_weight=narrow_out_weight, residual=residual, norm_gain=norm_gain, route_ids=route_ids, route_weights=route_weights, expert_gate=expert_gate, expert_up=expert_up, expert_down=expert_down, shared_gate=shared_gate, shared_up=shared_up, shared_down=shared_down)


THETA = 10000.0
EPS = 1e-06

def stored(values):
    return lax.optimization_barrier(values.astype(jnp.bfloat16))

def rotate(values, positions):
    half_width = values.shape[-1] // 2
    frequency = THETA ** (-2.0 * jnp.arange(half_width, dtype=jnp.float32) / values.shape[-1])
    angles = positions.astype(jnp.float32)[:, None] * frequency[None, :]
    if values.ndim == 3:
        angles = angles[:, None, :]
    cosine = jnp.cos(angles)
    sine_part = jnp.sin(angles)
    as_float = values.astype(jnp.float32)
    first_half = as_float[..., :half_width]
    second_half = as_float[..., half_width:]
    return stored(jnp.concatenate([first_half * cosine - second_half * sine_part, second_half * cosine + first_half * sine_part], axis=-1))

def rms_scale(values, gain):
    as_float = values.astype(jnp.float32)
    scaled = as_float * lax.rsqrt(lax.optimization_barrier(jnp.mean(as_float * as_float, axis=-1, keepdims=True)) + EPS)
    return stored(scaled * gain)

def attend(queries, nope_width, key_nope, key_rot, values):
    token_count = queries.shape[0]
    scale = queries.shape[-1] ** (-0.5)
    query_nope = queries[..., :nope_width].astype(jnp.float32)
    query_rope = queries[..., nope_width:].astype(jnp.float32)
    keys_float = key_nope.astype(jnp.float32)
    rot_float = key_rot.astype(jnp.float32)
    values_float = values.astype(jnp.float32)
    key_pos = jnp.arange(token_count, dtype=jnp.int32)

    def one_block(block_index):
        first_row = (block_index * TOK_DEV).astype(jnp.int32)
        block_nope = lax.dynamic_slice_in_dim(query_nope, first_row, TOK_DEV, 0)
        block_rope = lax.dynamic_slice_in_dim(query_rope, first_row, TOK_DEV, 0)
        scores = jnp.einsum('qhd,khd->hqk', block_nope, keys_float)
        scores = (scores + jnp.einsum('qhr,kr->hqk', block_rope, rot_float)) * scale
        query_pos = first_row + jnp.arange(TOK_DEV, dtype=jnp.int32)
        allowed = (query_pos[:, None] >= key_pos[None, :])[None]
        scores = jnp.where(allowed, scores, -jnp.inf)
        row_peak = lax.optimization_barrier(jnp.max(scores, axis=-1, keepdims=True))
        expo = jnp.exp(scores - row_peak)
        row_total = lax.optimization_barrier(jnp.sum(expo, axis=-1))
        probs = stored(expo).astype(jnp.float32)
        mixed = jnp.einsum('hqk,khv->qhv', probs, values_float)
        return stored(mixed / row_total.T[:, :, None])
    blocks = lax.map(one_block, jnp.arange(token_count // TOK_DEV, dtype=jnp.int32))
    return blocks.reshape(token_count, queries.shape[1], values.shape[-1])

def reference(wide_queries, narrow_queries, kv_latent, rope_key, latent_gain, wide_kv_weight, narrow_kv_weight, wide_out_weight, narrow_out_weight, residual, norm_gain, route_ids, route_weights, expert_gate, expert_up, expert_down, shared_gate, shared_up, shared_down):
    token_count = residual.shape[0]
    positions = jnp.arange(token_count, dtype=jnp.int32)
    wide_q = wide_queries.reshape(token_count, WIDE_HEADS, WIDE_NOPE + ROPE_DIM)
    wide_q = jnp.concatenate([wide_q[..., :WIDE_NOPE], rotate(wide_q[..., WIDE_NOPE:], positions)], axis=-1)
    narrow_q = narrow_queries.reshape(token_count, NARROW_HEADS, NARROW_NOPE + ROPE_DIM)
    narrow_q = jnp.concatenate([narrow_q[..., :NARROW_NOPE], rotate(narrow_q[..., NARROW_NOPE:], positions)], axis=-1)
    key_rot = rotate(rope_key, positions)
    latent = rms_scale(kv_latent, latent_gain)
    wide_kv = stored(jnp.dot(latent, wide_kv_weight, preferred_element_type=jnp.float32))
    wide_kv = wide_kv.reshape(token_count, WIDE_HEADS, WIDE_NOPE + WIDE_VALUE)
    narrow_kv = stored(jnp.dot(latent, narrow_kv_weight, preferred_element_type=jnp.float32))
    narrow_kv = narrow_kv.reshape(token_count, NARROW_HEADS, NARROW_NOPE + NARROW_VALUE)
    wide_att = attend(wide_q, WIDE_NOPE, wide_kv[..., :WIDE_NOPE], key_rot, wide_kv[..., WIDE_NOPE:])
    narrow_att = attend(narrow_q, NARROW_NOPE, narrow_kv[..., :NARROW_NOPE], key_rot, narrow_kv[..., NARROW_NOPE:])
    wide_per = WIDE_HEADS // N_TP
    narrow_per = NARROW_HEADS // N_TP
    wide_proj = wide_out_weight.reshape(WIDE_HEADS, WIDE_VALUE, D_MODEL).astype(jnp.float32)
    narrow_proj = narrow_out_weight.reshape(NARROW_HEADS, NARROW_VALUE, D_MODEL).astype(jnp.float32)
    proj_total = jnp.zeros((token_count, D_MODEL), jnp.float32)
    for group_index in range(N_TP):
        wide_slice = slice(group_index * wide_per, (group_index + 1) * wide_per)
        narrow_slice = slice(group_index * narrow_per, (group_index + 1) * narrow_per)
        partial_sum = jnp.einsum('thv,hvd->td', wide_att[:, wide_slice].astype(jnp.float32), wide_proj[wide_slice])
        partial_sum = partial_sum + jnp.einsum('thv,hvd->td', narrow_att[:, narrow_slice].astype(jnp.float32), narrow_proj[narrow_slice])
        proj_total = proj_total + stored(partial_sum).astype(jnp.float32)
    attn_proj = stored(proj_total)
    stream = stored(residual.astype(jnp.float32) + attn_proj.astype(jnp.float32))
    normed = rms_scale(stream, norm_gain)
    unit_per = EXPERT_FF // N_TP
    shared_hidden = stored(jax.nn.silu(jnp.dot(normed, shared_gate, preferred_element_type=jnp.float32)) * jnp.dot(normed, shared_up, preferred_element_type=jnp.float32))
    shared_total = jnp.zeros((token_count, D_MODEL), jnp.float32)
    for group_index in range(N_TP):
        unit_slice = slice(group_index * unit_per, (group_index + 1) * unit_per)
        shared_total = shared_total + stored(jnp.dot(shared_hidden[:, unit_slice], shared_down[unit_slice], preferred_element_type=jnp.float32)).astype(jnp.float32)
    shared_out = stored(shared_total)
    flat_ids = route_ids.reshape(-1)
    flat_weights = route_weights.reshape(-1)
    copy_count = token_count * TOP_K
    slot_count = N_SP * CAPACITY

    def visit_expert(routed_acc, expert):
        picked = jnp.nonzero(flat_ids == expert, size=slot_count, fill_value=copy_count)[0].astype(jnp.int32)
        is_live = picked < copy_count
        safe_pick = jnp.minimum(picked, copy_count - 1).astype(jnp.int32)
        token_index = (safe_pick // TOP_K).astype(jnp.int32)
        picked_rows = normed[token_index]
        hidden_units = stored(jax.nn.silu(jnp.dot(picked_rows, expert_gate[expert], preferred_element_type=jnp.float32)) * jnp.dot(picked_rows, expert_up[expert], preferred_element_type=jnp.float32))
        down_weight = expert_down[expert]
        expert_total = jnp.zeros((slot_count, D_MODEL), jnp.float32)
        for group_index in range(N_TP):
            unit_slice = slice(group_index * unit_per, (group_index + 1) * unit_per)
            expert_total = expert_total + stored(jnp.dot(hidden_units[:, unit_slice], down_weight[unit_slice], preferred_element_type=jnp.float32)).astype(jnp.float32)
        expert_result = stored(expert_total).astype(jnp.float32)
        weighting = jnp.where(is_live, flat_weights[safe_pick], 0.0)
        routed_acc = routed_acc.at[token_index].add(weighting[:, None] * expert_result)
        return (routed_acc, None)
    routed, _ = lax.scan(visit_expert, jnp.zeros((token_count, D_MODEL), jnp.float32), jnp.arange(EXPERTS, dtype=jnp.int32))
    return (stream.astype(jnp.float32) + shared_out.astype(jnp.float32) + routed).astype(jnp.bfloat16)
```

```python
import functools

import jax
import jax.numpy as jnp
from jax import lax
from jax.experimental import pallas as pl
from jax.experimental.pallas import tpu as pltpu
from jax.sharding import Mesh
from jax.sharding import PartitionSpec as P

D_MODEL = 2048
THETA = 10000.0
EPS = 1e-06
FLOOR = -1e30
SP = ("z", "c")
N_SP = 32
N_TP = 16
TOK = 64
SLOTS = 192
F32 = jnp.float32
BF = jnp.bfloat16

LANE_POS, LANE_HI, LANE_LO, LANE_FLAG = 64, 65, 66, 67


def iota(shape, dim):
    return lax.broadcasted_iota(jnp.int32, shape, dim)


def div6(v):
    return (v * 10923) >> 16


def div3(v):
    return (v * 21846) >> 16


def dot(a, b):
    return jnp.dot(a, b, preferred_element_type=F32)


def dot_nt(a, b):
    return lax.dot_general(a, b, (((1,), (1,)), ((), ())), preferred_element_type=F32)


def dot_tn(a, b):
    return lax.dot_general(a, b, (((0,), (0,)), ((), ())), preferred_element_type=F32)


def picks(mask):
    return jnp.where(mask, 1.0, 0.0).astype(BF)


def lane_value(block, lane):
    return jnp.sum(jnp.where(iota(block.shape, 1) == lane, block, 0.0), axis=1, keepdims=True)


def slot_rows(arrived):
    row, col = iota((SLOTS, 256), 0), iota((SLOTS, 256), 1)
    source = div6(row)
    return picks(col == source * 8 + (row - source * 6))


def pack_kernel(tp_ref, q_ref, rope_ref, lat_ref, gain_ref, res_ref, ids_ref, idst_ref, w_ref, cos_ref, sin_ref, out_ref, sel_ref):
    t = tp_ref[0]
    cos, sin = cos_ref[...], sin_ref[...]
    src, dst = iota((128, 128), 0), iota((128, 128), 1)
    swap = picks(src == dst + jnp.where((dst & 16) == 0, 16, -16))

    def turned(block):
        return (block.astype(F32) * cos + dot(block, swap) * sin).astype(BF)

    q_nope = q_ref[:, :128]
    q_rest = turned(q_ref[:, 128:])
    rope = turned(rope_ref[...])
    lat = lat_ref[...].astype(F32)
    scaled = lat * lax.rsqrt(jnp.mean(lat * lat, axis=1, keepdims=True) + EPS)
    normed = (scaled * gain_ref[...]).astype(BF)
    res = res_ref[:, pl.ds(pl.multiple_of(t * 128, 128), 128)]

    earlier = iota((TOK, TOK), 0) < iota((TOK, TOK), 1)
    row, tok = iota((256, TOK), 0), iota((256, TOK), 1)
    dest, place = row >> 3, row & 7
    lane = iota((TOK, 128), 1)
    local_pos = iota((TOK, 128), 0).astype(F32)
    selects, sides = [], []
    for k in range(2):
        named = idst_ref[k : k + 1, :]
        same = jnp.where(((ids_ref[:, 0:1] == named) | (ids_ref[:, 1:2] == named)) & earlier, 1, 0)
        slot = named * 3 + jnp.sum(same, axis=0, keepdims=True)
        selects.append(picks((slot == dest * 6 + place) & (place < 6)))
        w = w_ref[:, k : k + 1]
        w_hi = w.astype(BF).astype(F32)
        side = jnp.where(lane == LANE_POS, local_pos, 0.0)
        side = jnp.where(lane == LANE_HI, w_hi, side)
        side = jnp.where(lane == LANE_LO, w - w_hi, side)
        side = jnp.where(lane == LANE_FLAG, 1.0 - k, side)
        sides.append(side.astype(BF))
    either = selects[0] + selects[1]
    sel_ref[...] = either
    first = (dest & 1) * 32 + t * 2
    token_row = picks((place >= 6) & (tok == first + place - 6))
    rope_row = picks((place < 2) & (tok == first + place))
    lat_part = dot(token_row, normed)
    out_ref[:, :128] = (dot(either, q_nope) + lat_part[:, :128]).astype(BF)
    out_ref[:, 128:256] = (dot(either, q_rest) + lat_part[:, 128:256]).astype(BF)
    out_ref[:, 256:384] = (dot(either, res) + lat_part[:, 256:384]).astype(BF)
    side = dot(selects[0], sides[0]) + dot(selects[1], sides[1]) + dot(rope_row, rope)
    out_ref[:, 384:] = (side + lat_part[:, 384:]).astype(BF)


def spread_kernel(arr_ref, out_ref):
    row, col = iota((TOK, 256), 0), iota((TOK, 256), 1)
    base = (row >> 1) * 8 + (row & 1)
    lat = dot(picks(col == base + 6), arr_ref[...]).astype(BF)
    side = arr_ref[:, 384:]
    packed = jnp.zeros((16, 128), F32)
    for b in range(4):
        near, far = iota((16, 256), 0) + 16 * b, iota((16, 256), 1)
        here = dot(picks(far == (near >> 1) * 8 + (near & 1)), side).astype(BF)
        src, dst = iota((128, 128), 0), iota((128, 128), 1)
        packed = packed + dot(here, picks((src < 32) & (dst == src + 32 * b)))
    packed = packed.astype(BF)
    for copy in range(N_TP):
        for f in range(4):
            out_ref[copy, f * TOK : (f + 1) * TOK, :] = lat[:, f * 128 : (f + 1) * 128]
        out_ref[copy, 4 * TOK :, :] = packed


def keys_kernel(lat_ref, wide_ref, narrow_ref, out_ref):
    rows = N_TP * TOK
    wide = jnp.zeros((rows, 256), F32)
    narrow = jnp.zeros((rows, 128), F32)
    for f in range(4):
        part = lat_ref[:, f * TOK : (f + 1) * TOK, :].reshape(rows, 128)
        wide = wide + dot(part, wide_ref[f * 128 : (f + 1) * 128, :])
        narrow = narrow + dot(part, narrow_ref[f * 128 : (f + 1) * 128, :])
    wide, narrow = wide.astype(BF), narrow.astype(BF)
    packed = lat_ref[:, 4 * TOK :, :].reshape(256, 128)
    src, dst = iota((128, 128), 0), iota((128, 128), 1)
    pieces = []
    for b in range(4):
        moved = dot(packed, picks((dst >= 96) & (src == dst - 96 + 32 * b)))
        pieces.append(moved.astype(BF).reshape(N_TP, 16, 128))
    rope = jnp.concatenate(pieces, axis=1).reshape(rows, 128)
    out_ref[0] = wide[:, :128]
    out_ref[1] = wide[:, 128:]
    shifted = dot(narrow, picks((src < 64) & (dst == src + 32)))
    out_ref[2] = (shifted + rope.astype(F32)).astype(BF)
    out_ref[3] = dot(narrow, picks((src >= 64) & (dst == src - 64))).astype(BF)


def attend_kernel(core_ref, arr_ref, own_ref, other_ref, wide_out_ref, narrow_out_ref, out_ref):
    core = core_ref[0]
    pick = slot_rows(arr_ref)
    q = dot(pick, arr_ref[:, :256]).astype(BF)
    side = dot(pick, arr_ref[:, 384:])
    row_pos = div6(iota((SLOTS, 1), 0)) * TOK + lane_value(side, LANE_POS).astype(jnp.int32)
    src, dst = iota((128, 128), 0), iota((128, 128), 1)
    q_rest = q[:, 128:]
    wide_q = jnp.concatenate([q[:, :128], dot(q_rest, picks((src < 32) & (dst == src + 96))).astype(BF)], axis=1)
    narrow_q = jnp.where(iota((SLOTS, 128), 1) >= 32, q_rest.astype(F32), 0.0).astype(BF)
    rows = N_TP * TOK
    n = iota((1, rows), 1)
    near = ((n & 63) >> 1) * TOK + (n >> 6) * 2 + (n & 1)
    wide_scores, narrow_scores, masks = [], [], []
    for half, ref in ((core, own_ref), (1 - core, other_ref)):
        allowed = near + half * 32 <= row_pos
        keys = jnp.concatenate([ref[0], ref[2]], axis=1)
        wide = dot_nt(wide_q, keys) * (160 ** -0.5)
        narrow = dot_nt(narrow_q, ref[2]) * (96 ** -0.5)
        wide_scores.append(jnp.where(allowed, wide, FLOOR))
        narrow_scores.append(jnp.where(allowed, narrow, FLOOR))

    def mixed(scores, at):
        peak = jnp.maximum(*[jnp.max(s, axis=1, keepdims=True) for s in scores])
        total, summed = 0.0, 0.0
        for s, ref in zip(scores, (own_ref, other_ref)):
            e = jnp.exp(s - peak)
            total = total + jnp.sum(e, axis=1, keepdims=True)
            summed = summed + dot(e.astype(BF), ref[at])
        return (summed / total).astype(BF)

    wide_att = mixed(wide_scores, 1)
    narrow_att = mixed(narrow_scores, 3)[:, :64]
    for piece in range(N_TP):
        cols = slice(piece * 128, (piece + 1) * 128)
        out_ref[piece] = (dot(wide_att, wide_out_ref[:, cols]) + dot(narrow_att, narrow_out_ref[:, cols])).astype(BF)


def stream_kernel(part_ref, arr_ref, out_ref):
    total = jnp.zeros((SLOTS, 128), F32)
    for piece in range(N_TP):
        total = total + part_ref[piece].astype(F32)
    res = dot(slot_rows(arr_ref), arr_ref[:, 256:384])
    stream = (res + total.astype(BF).astype(F32)).astype(BF)
    for copy in range(N_TP):
        out_ref[copy] = stream


def expert_kernel(x_ref, arr_ref, gain_ref, eg_ref, eu_ref, ed_ref, sg_ref, su_ref, sd_ref, out_ref):
    squares = jnp.zeros((SLOTS, 128), F32)
    for piece in range(N_TP):
        x = x_ref[piece].astype(F32)
        squares = squares + x * x
    scale = lax.rsqrt(jnp.sum(squares, axis=1, keepdims=True) * (1.0 / D_MODEL) + EPS)
    zero = jnp.zeros((SLOTS, 64), F32)
    gates, ups = [zero] * 3, [zero] * 3
    for piece in range(N_TP):
        cols = slice(piece * 128, (piece + 1) * 128)
        x = (x_ref[piece].astype(F32) * scale * gain_ref[:, cols]).astype(BF)
        for e in range(2):
            gates[e] = gates[e] + dot(x, eg_ref[e, cols, :])
            ups[e] = ups[e] + dot(x, eu_ref[e, cols, :])
        gates[2] = gates[2] + dot(x, sg_ref[cols, :])
        ups[2] = ups[2] + dot(x, su_ref[cols, :])
    hidden = [((g / (1.0 + jnp.exp(-g))) * u).astype(BF) for g, u in zip(gates, ups)]
    side = dot(slot_rows(arr_ref), arr_ref[:, 384:])
    weight = lane_value(side, LANE_HI) + lane_value(side, LANE_LO)
    flag = lane_value(side, LANE_FLAG)
    row = iota((SLOTS, 1), 0)
    second = div3(row) & 1
    first_hidden = jnp.where(second == 0, hidden[0].astype(F32), 0.0).astype(BF)
    second_hidden = jnp.where(second == 1, hidden[1].astype(F32), 0.0).astype(BF)
    for piece in range(N_TP):
        cols = slice(piece * 128, (piece + 1) * 128)
        routed = dot(first_hidden, ed_ref[0, :, cols]) + dot(second_hidden, ed_ref[1, :, cols])
        shared = dot(hidden[2], sd_ref[:, cols])
        out_ref[piece] = (weight * routed + flag * shared).astype(BF)


def give_back_kernel(part_ref, stream_ref, arr_ref, out_ref):
    total = jnp.zeros((SLOTS, 128), F32)
    for piece in range(N_TP):
        total = total + part_ref[piece].astype(F32)
    pick = slot_rows(arr_ref)
    flag = lane_value(dot(pick, arr_ref[:, 384:]), LANE_FLAG)
    total = (total + flag * stream_ref[...].astype(F32)).astype(BF)
    out_ref[...] = dot_tn(pick, total).astype(BF)


def finish_kernel(sel_ref, back_ref, out_ref):
    out_ref[...] = dot_tn(sel_ref[...], back_ref[...]).astype(BF)


VMEM = pl.BlockSpec(memory_space=pltpu.VMEM)
SMEM = pl.BlockSpec(memory_space=pltpu.SMEM)


def run(kernel, outs, *args, scalars=0):
    shapes = [jax.ShapeDtypeStruct(s, BF) for s in outs]
    got = pl.pallas_call(
        kernel,
        out_shape=shapes,
        in_specs=[SMEM] * scalars + [VMEM] * (len(args) - scalars),
        out_specs=[VMEM] * len(outs),
        name=kernel.__name__,
    )(*args)
    return got[0] if len(outs) == 1 else got


def swap_all(values, axes):
    return lax.all_to_all(values, axes, split_axis=0, concat_axis=0, tiled=True)


def local(
    wide_queries,
    narrow_queries,
    kv_latent,
    rope_key,
    latent_gain,
    wide_kv_weight,
    narrow_kv_weight,
    wide_out_weight,
    narrow_out_weight,
    residual,
    norm_gain,
    route_ids,
    route_weights,
    expert_gate,
    expert_up,
    expert_down,
    shared_gate,
    shared_up,
    shared_down,
):
    t = lax.axis_index("tp").astype(jnp.int32)[None]
    core = lax.axis_index("c").astype(jnp.int32)[None]
    lane = jnp.arange(128, dtype=jnp.int32)
    frequency = THETA ** (-2.0 * (lane % 16).astype(F32) / 32)
    positions = lax.axis_index(SP) * TOK + jnp.arange(TOK, dtype=jnp.int32)
    angles = positions.astype(F32)[:, None] * frequency[None, :]
    turning = ((lane < 32) | (lane >= 96))[None, :]
    cos = jnp.where(turning, jnp.cos(angles), 1.0)
    sign = jnp.where((lane & 16) == 0, -1.0, 1.0)[None, :]
    sin = jnp.where(turning, jnp.sin(angles) * sign, 0.0)
    queries = jnp.concatenate([wide_queries, narrow_queries], axis=1)
    rope = jnp.pad(rope_key, ((0, 0), (0, 96)))
    payload, chosen = run(
        pack_kernel, [(256, 512), (256, TOK)],
        t, queries, rope, kv_latent, latent_gain[None, :], residual, route_ids, route_ids.T, route_weights, cos, sin,
        scalars=1,
    )
    arrived = swap_all(payload.reshape(N_SP, 8, 512), SP).reshape(256, 512)
    latents = swap_all(run(spread_kernel, [(N_TP, 272, 128)], arrived), "tp")
    own = run(keys_kernel, [(4, N_TP * TOK, 128)], latents, wide_kv_weight, narrow_kv_weight)
    other = lax.ppermute(own, "c", [(0, 1), (1, 0)])
    partial = run(
        attend_kernel, [(N_TP, SLOTS, 128)], core, arrived, own, other, wide_out_weight, narrow_out_weight, scalars=1
    )
    copies = run(stream_kernel, [(N_TP, SLOTS, 128)], swap_all(partial, "tp"), arrived)
    rows = swap_all(copies, "tp")
    partial = run(
        expert_kernel, [(N_TP, SLOTS, 128)],
        rows, arrived, norm_gain[None, :], expert_gate, expert_up, expert_down, shared_gate, shared_up, shared_down,
    )
    back = run(give_back_kernel, [(256, 128)], swap_all(partial, "tp"), copies[0], arrived)
    back = swap_all(back.reshape(N_SP, 8, 128), SP).reshape(256, 128)
    return run(finish_kernel, [(TOK, 128)], chosen, back)


def solution(mesh):
    torus = Mesh(mesh.devices.reshape(16, 2, mesh.shape["tp"]), ("z", "c", "tp"))
    return jax.shard_map(
        local,
        mesh=torus,
        in_specs=(
            P(SP, "tp"),
            P(SP, "tp"),
            P(SP, None),
            P(SP, None),
            P(),
            P(None, "tp"),
            P(None, "tp"),
            P("tp", None),
            P("tp", None),
            P(SP, None),
            P(),
            P(SP, None),
            P(SP, None),
            P(SP, None, "tp"),
            P(SP, None, "tp"),
            P(SP, "tp", None),
            P(None, "tp"),
            P(None, "tp"),
            P("tp", None),
        ),
        out_specs=P(SP, "tp"),
        check_vma=False,
    )
```

```python
import functools

import jax
import jax.numpy as jnp
from jax import lax
from jax.experimental import pallas as pl
from jax.experimental.pallas import tpu as pltpu
from jax.sharding import Mesh
from jax.sharding import PartitionSpec as P

D_MODEL = 2048
THETA = 10000.0
EPS = 1e-06
FLOOR = -1e30
SP = ("z", "c")
N_SP = 32
N_TP = 16
TOK = 64
SLOTS = 192
F32 = jnp.float32
BF = jnp.bfloat16

LANE_POS, LANE_HI, LANE_LO, LANE_FLAG = 64, 65, 66, 67


def iota(shape, dim):
    return lax.broadcasted_iota(jnp.int32, shape, dim)


def div6(v):
    return (v * 10923) >> 16


def div3(v):
    return (v * 21846) >> 16


def dot(a, b):
    return jnp.dot(a, b, preferred_element_type=F32)


def dot_nt(a, b):
    return lax.dot_general(a, b, (((1,), (1,)), ((), ())), preferred_element_type=F32)


def dot_tn(a, b):
    return lax.dot_general(a, b, (((0,), (0,)), ((), ())), preferred_element_type=F32)


def exact_tn(a, b):
    return lax.dot_general(
        a, b, (((0,), (0,)), ((), ())), precision=lax.Precision.HIGHEST, preferred_element_type=F32
    )


def picks(mask):
    return jnp.where(mask, 1.0, 0.0).astype(BF)


def lane_value(block, lane):
    return jnp.sum(jnp.where(iota(block.shape, 1) == lane, block, 0.0), axis=1, keepdims=True)


def slot_rows():
    row, col = iota((SLOTS, 256), 0), iota((SLOTS, 256), 1)
    source = div6(row)
    return picks(col == source * 8 + (row - source * 6))


def pack_kernel(tp_ref, wide_ref, narrow_ref, rope_ref, lat_ref, gain_ref, res_ref, ids_ref, w_ref, cos_ref, sin_ref, out_ref, sel_ref):
    t = tp_ref[0]
    src, dst = iota((16, 128), 0), iota((16, 128), 1)
    turning = (dst < 32) | (dst >= 96)
    spread = jnp.where(turning & ((dst & 15) == src), 1.0, 0.0)
    cos = exact_tn(cos_ref[...], spread) + jnp.where((iota((TOK, 128), 1) >= 32) & (iota((TOK, 128), 1) < 96), 1.0, 0.0)
    sin = exact_tn(sin_ref[...], jnp.where((dst & 16) == 0, -spread, spread))
    src, dst = iota((128, 128), 0), iota((128, 128), 1)
    swap = picks(src == dst + jnp.where((dst & 16) == 0, 16, -16))

    def turned(block):
        return (block.astype(F32) * cos + dot(block, swap) * sin).astype(BF)

    first, after = picks(src == dst), picks(src + 32 == dst)
    q_rest = turned((dot(wide_ref[:, 128:], first[:32]) + dot(narrow_ref[...], after[:96])).astype(BF))
    rope = turned(dot_tn(rope_ref[...], first[:32]).astype(BF))
    lat = lat_ref[...].astype(F32)
    scaled = lat * lax.rsqrt(jnp.mean(lat * lat, axis=1, keepdims=True) + EPS)
    normed = (scaled * gain_ref[...]).astype(BF)
    res = res_ref[:, pl.ds(pl.multiple_of(t * 128, 128), 128)]

    before = picks(iota((TOK, TOK), 0) < iota((TOK, TOK), 1))
    named = [jnp.where(ids_ref[k : k + 1, :] == iota((TOK, TOK), 0), 1.0, 0.0) for k in range(2)]
    rank = dot((named[0] + named[1]).astype(BF), before)
    row, tok = iota((256, TOK), 0), iota((256, TOK), 1)
    dest, place = row >> 3, row & 7
    selects, high, low = [], 0.0, 0.0
    for k in range(2):
        slot = ids_ref[k : k + 1, :] * 3 + jnp.sum(named[k] * rank, axis=0, keepdims=True).astype(jnp.int32)
        mask = (slot == dest * 6 + place) & (place < 6)
        selects.append(picks(mask))
        w = w_ref[k : k + 1, :]
        w_hi = w.astype(BF).astype(F32)
        high = high + jnp.where(mask, w_hi, 0.0)
        low = low + jnp.where(mask, w - w_hi, 0.0)
    either = selects[0] + selects[1]
    sel_ref[...] = either
    start = (dest & 1) * 32 + t * 2
    token_row = picks((place >= 6) & (tok == start + place - 6))
    rope_row = picks((place < 2) & (tok == start + place))
    lat_part = dot(token_row, normed)
    out_ref[:, :128] = (dot(either, wide_ref[:, :128]) + lat_part[:, :128]).astype(BF)
    out_ref[:, 128:256] = (dot(either, q_rest) + lat_part[:, 128:256]).astype(BF)
    out_ref[:, 256:384] = (dot(either, res) + lat_part[:, 256:384]).astype(BF)
    lane, token = iota((TOK, 128), 1), iota((TOK, 128), 0).astype(F32)
    side = dot(either, jnp.where(lane == LANE_POS, token, 0.0).astype(BF))
    side = side + dot(high.astype(BF), picks(lane == LANE_HI)) + dot(low.astype(BF), picks(lane == LANE_LO))
    side = side + dot(selects[0], picks(lane == LANE_FLAG)) + dot(rope_row, rope)
    out_ref[:, 384:] = (side + lat_part[:, 384:]).astype(BF)


def slots_kernel(arr_ref, out_ref):
    out_ref[...] = dot(slot_rows(), arr_ref[...]).astype(BF)


def spread_kernel(arr_ref, out_ref):
    row, col = iota((TOK, 256), 0), iota((TOK, 256), 1)
    base = (row >> 1) * 8 + (row & 1)
    lat = dot(picks(col == base + 6), arr_ref[...]).astype(BF)
    side = arr_ref[:, 384:]
    packed = jnp.zeros((16, 128), F32)
    for b in range(4):
        near, far = iota((16, 256), 0) + 16 * b, iota((16, 256), 1)
        here = dot(picks(far == (near >> 1) * 8 + (near & 1)), side).astype(BF)
        src, dst = iota((128, 128), 0), iota((128, 128), 1)
        packed = packed + dot(here, picks((src < 32) & (dst == src + 32 * b)))
    packed = packed.astype(BF)
    for copy in range(N_TP):
        for f in range(4):
            out_ref[copy, f * TOK : (f + 1) * TOK, :] = lat[:, f * 128 : (f + 1) * 128]
        out_ref[copy, 4 * TOK :, :] = packed


def keys_kernel(lat_ref, wide_ref, narrow_ref, out_ref):
    rows = N_TP * TOK
    wide = jnp.zeros((rows, 256), F32)
    narrow = jnp.zeros((rows, 128), F32)
    for f in range(4):
        part = lat_ref[:, f * TOK : (f + 1) * TOK, :].reshape(rows, 128)
        wide = wide + dot(part, wide_ref[f * 128 : (f + 1) * 128, :])
        narrow = narrow + dot(part, narrow_ref[f * 128 : (f + 1) * 128, :])
    wide, narrow = wide.astype(BF), narrow.astype(BF)
    packed = lat_ref[:, 4 * TOK :, :].reshape(256, 128)
    src, dst = iota((128, 128), 0), iota((128, 128), 1)
    pieces = []
    for b in range(4):
        moved = dot(packed, picks((dst >= 96) & (src == dst - 96 + 32 * b)))
        pieces.append(moved.astype(BF).reshape(N_TP, 16, 128))
    rope = jnp.concatenate(pieces, axis=1).reshape(rows, 128)
    out_ref[0] = wide[:, :128]
    out_ref[1] = wide[:, 128:]
    shifted = dot(narrow, picks((src < 64) & (dst == src + 32)))
    out_ref[2] = (shifted + rope.astype(F32)).astype(BF)
    out_ref[3] = dot(narrow, picks((src >= 64) & (dst == src - 64))).astype(BF)


def attend_kernel(core_ref, slot_ref, own_ref, other_ref, wide_out_ref, narrow_out_ref, out_ref):
    core = core_ref[0]
    q = slot_ref[:, :256]
    side = slot_ref[:, 384:].astype(F32)
    row_pos = div6(iota((SLOTS, 1), 0)) * TOK + lane_value(side, LANE_POS).astype(jnp.int32)
    src, dst = iota((128, 128), 0), iota((128, 128), 1)
    q_rest = q[:, 128:]
    wide_q = jnp.concatenate([q[:, :128], dot(q_rest, picks((src < 32) & (dst == src + 96))).astype(BF)], axis=1)
    narrow_q = jnp.where(iota((SLOTS, 128), 1) >= 32, q_rest.astype(F32), 0.0).astype(BF)
    rows = N_TP * TOK
    n = iota((1, rows), 1)
    near = ((n & 63) >> 1) * TOK + (n >> 6) * 2 + (n & 1)
    wide_scores, narrow_scores, masks = [], [], []
    for half, ref in ((core, own_ref), (1 - core, other_ref)):
        allowed = near + half * 32 <= row_pos
        keys = jnp.concatenate([ref[0], ref[2]], axis=1)
        wide = dot_nt(wide_q, keys) * (160 ** -0.5)
        narrow = dot_nt(narrow_q, ref[2]) * (96 ** -0.5)
        wide_scores.append(jnp.where(allowed, wide, FLOOR))
        narrow_scores.append(jnp.where(allowed, narrow, FLOOR))

    def mixed(scores, at):
        peak = jnp.maximum(*[jnp.max(s, axis=1, keepdims=True) for s in scores])
        total, summed = 0.0, 0.0
        for s, ref in zip(scores, (own_ref, other_ref)):
            e = jnp.exp(s - peak)
            total = total + jnp.sum(e, axis=1, keepdims=True)
            summed = summed + dot(e.astype(BF), ref[at])
        return (summed / total).astype(BF)

    wide_att = mixed(wide_scores, 1)
    narrow_att = mixed(narrow_scores, 3)[:, :64]
    for piece in range(N_TP):
        cols = slice(piece * 128, (piece + 1) * 128)
        out_ref[piece] = (dot(wide_att, wide_out_ref[:, cols]) + dot(narrow_att, narrow_out_ref[:, cols])).astype(BF)


def stream_kernel(part_ref, slot_ref, out_ref):
    total = jnp.zeros((SLOTS, 128), F32)
    for piece in range(N_TP):
        total = total + part_ref[piece].astype(F32)
    stream = (slot_ref[:, 256:384].astype(F32) + total.astype(BF).astype(F32)).astype(BF)
    for copy in range(N_TP):
        out_ref[copy] = stream


def expert_kernel(x_ref, slot_ref, gain_ref, eg_ref, eu_ref, ed_ref, sg_ref, su_ref, sd_ref, out_ref):
    squares = jnp.zeros((SLOTS, 128), F32)
    for piece in range(N_TP):
        x = x_ref[piece].astype(F32)
        squares = squares + x * x
    scale = lax.rsqrt(jnp.sum(squares, axis=1, keepdims=True) * (1.0 / D_MODEL) + EPS)
    into = jnp.zeros((SLOTS, 384), F32)
    for pair in range(N_TP // 2):
        cols = slice(pair * 256, (pair + 1) * 256)
        x = jnp.concatenate([x_ref[2 * pair], x_ref[2 * pair + 1]], axis=1).astype(F32)
        x = (x * scale * gain_ref[:, cols]).astype(BF)
        weights = [eg_ref[0, :, cols], eg_ref[1, :, cols], sg_ref[:, cols], eu_ref[0, :, cols], eu_ref[1, :, cols], su_ref[:, cols]]
        into = into + dot_nt(x, jnp.concatenate(weights, axis=0))
    gate, up = into[:, :192], into[:, 192:]
    hidden = (gate / (1.0 + jnp.exp(-gate))) * up
    side = slot_ref[:, 384:].astype(F32)
    weight = lane_value(side, LANE_HI) + lane_value(side, LANE_LO)
    flag = lane_value(side, LANE_FLAG)
    owner = div3(iota((SLOTS, 128), 0)) & 1
    routed_hidden = jnp.where(owner == (iota((SLOTS, 128), 1) >> 6), hidden[:, :128], 0.0).astype(BF)
    shared_hidden = hidden[:, 128:].astype(BF)
    for piece in range(N_TP // 2):
        cols = slice(piece * 256, (piece + 1) * 256)
        routed = dot(routed_hidden, ed_ref[:, cols])
        shared = dot(shared_hidden, sd_ref[:, cols])
        both = (weight * routed + flag * shared).astype(BF)
        out_ref[2 * piece] = both[:, :128]
        out_ref[2 * piece + 1] = both[:, 128:]


def give_back_kernel(part_ref, stream_ref, slot_ref, out_ref):
    total = jnp.zeros((SLOTS, 128), F32)
    for piece in range(N_TP):
        total = total + part_ref[piece].astype(F32)
    flag = lane_value(slot_ref[:, 384:].astype(F32), LANE_FLAG)
    total = (total + flag * stream_ref[0].astype(F32)).astype(BF)
    out_ref[...] = dot_tn(slot_rows(), total).astype(BF)


def finish_kernel(sel_ref, back_ref, out_ref):
    out_ref[...] = dot_tn(sel_ref[...], back_ref[...]).astype(BF)


VMEM = pl.BlockSpec(memory_space=pltpu.VMEM)
SMEM = pl.BlockSpec(memory_space=pltpu.SMEM)


def run(kernel, outs, *args, scalars=0, plain=0, spread=True):
    placed = [pltpu.with_memory_space_constraint(a, pltpu.VMEM) for a in args[max(scalars, plain) :]]
    args = [*args[: max(scalars, plain)], *placed]
    return pl.pallas_call(
        kernel,
        out_shape=[pltpu.VMEM(shape, BF) for shape in outs] if spread else jax.ShapeDtypeStruct(outs[0], BF),
        in_specs=[SMEM] * scalars + [VMEM] * (len(args) - scalars),
        out_specs=[VMEM] * len(outs) if spread else VMEM,
        compiler_params=pltpu.CompilerParams(vmem_limit_bytes=24 << 20),
        name=kernel.__name__,
    )(*args)


def swap_all(values, axes):
    return lax.all_to_all(values, axes, split_axis=0, concat_axis=0, tiled=True)


def local(
    wide_queries,
    narrow_queries,
    kv_latent,
    rope_key,
    latent_gain,
    wide_kv_weight,
    narrow_kv_weight,
    wide_out_weight,
    narrow_out_weight,
    residual,
    norm_gain,
    route_ids,
    route_weights,
    expert_gate,
    expert_up,
    expert_down,
    shared_gate,
    shared_up,
    shared_down,
):
    t = lax.axis_index("tp").astype(jnp.int32)[None]
    core = lax.axis_index("c").astype(jnp.int32)[None]
    frequency = THETA ** (-2.0 * jnp.arange(16, dtype=F32) / 32)
    positions = lax.axis_index(SP) * TOK + jnp.arange(TOK, dtype=jnp.int32)
    angles = frequency[:, None] * positions.astype(F32)[None, :]
    payload, chosen = run(
        pack_kernel, [(256, 512), (256, TOK)],
        t, wide_queries, narrow_queries, rope_key.T, kv_latent, latent_gain[None, :], residual,
        route_ids.T, route_weights.T, jnp.cos(angles), jnp.sin(angles),
        scalars=1,
        plain=9,
    )
    arrived = swap_all(payload.reshape(N_SP, 8, 512), SP).reshape(256, 512)
    (spread,) = run(spread_kernel, [(N_TP, 272, 128)], arrived)
    latents = swap_all(spread, "tp")
    (slots,) = run(slots_kernel, [(SLOTS, 512)], arrived)
    (own,) = run(keys_kernel, [(4, N_TP * TOK, 128)], latents, wide_kv_weight, narrow_kv_weight)
    other = lax.ppermute(own, "c", [(0, 1), (1, 0)])
    (partial,) = run(
        attend_kernel, [(N_TP, SLOTS, 128)], core, slots, own, other, wide_out_weight, narrow_out_weight, scalars=1
    )
    (copies,) = run(stream_kernel, [(N_TP, SLOTS, 128)], swap_all(partial, "tp"), slots)
    rows = swap_all(copies, "tp")
    (partial,) = run(
        expert_kernel, [(N_TP, SLOTS, 128)],
        rows, slots, norm_gain[None, :],
        expert_gate.swapaxes(1, 2), expert_up.swapaxes(1, 2), expert_down.reshape(128, D_MODEL),
        shared_gate.T, shared_up.T, shared_down,
    )
    (back,) = run(give_back_kernel, [(256, 128)], swap_all(partial, "tp"), copies, slots)
    back = swap_all(back.reshape(N_SP, 8, 128), SP).reshape(256, 128)
    return run(finish_kernel, [(TOK, 128)], chosen, back, spread=False)


def solution(mesh):
    torus = Mesh(mesh.devices.reshape(16, 2, mesh.shape["tp"]), ("z", "c", "tp"))
    return jax.shard_map(
        local,
        mesh=torus,
        in_specs=(
            P(SP, "tp"),
            P(SP, "tp"),
            P(SP, None),
            P(SP, None),
            P(),
            P(None, "tp"),
            P(None, "tp"),
            P("tp", None),
            P("tp", None),
            P(SP, None),
            P(),
            P(SP, None),
            P(SP, None),
            P(SP, None, "tp"),
            P(SP, None, "tp"),
            P(SP, "tp", None),
            P(None, "tp"),
            P(None, "tp"),
            P("tp", None),
        ),
        out_specs=P(SP, "tp"),
        check_vma=False,
    )
```

```python
import functools

import jax
import jax.numpy as jnp
from jax import lax
from jax.experimental import pallas as pl
from jax.experimental.pallas import tpu as pltpu
from jax.sharding import Mesh
from jax.sharding import PartitionSpec as P

D_MODEL = 2048
THETA = 10000.0
EPS = 1e-06
FLOOR = -1e30
SP = ("z", "c")
N_SP = 32
N_TP = 16
TOK = 64
SLOTS = 192
F32 = jnp.float32
BF = jnp.bfloat16

LANE_POS, LANE_HI, LANE_LO, LANE_FLAG = 64, 65, 66, 67


def iota(shape, dim):
    return lax.broadcasted_iota(jnp.int32, shape, dim)


def div6(v):
    return (v * 10923) >> 16


def div3(v):
    return (v * 21846) >> 16


def dot(a, b):
    return jnp.dot(a, b, preferred_element_type=F32)


def dot_nt(a, b):
    return lax.dot_general(a, b, (((1,), (1,)), ((), ())), preferred_element_type=F32)


def dot_tn(a, b):
    return lax.dot_general(a, b, (((0,), (0,)), ((), ())), preferred_element_type=F32)


def exact_tn(a, b):
    return lax.dot_general(
        a, b, (((0,), (0,)), ((), ())), precision=lax.Precision.HIGHEST, preferred_element_type=F32
    )


def picks(mask):
    return jnp.where(mask, 1.0, 0.0).astype(BF)


def lane_value(block, lane):
    return jnp.sum(jnp.where(iota(block.shape, 1) == lane, block, 0.0), axis=1, keepdims=True)


def slot_rows():
    row, col = iota((SLOTS, 256), 0), iota((SLOTS, 256), 1)
    source = div6(row)
    return picks(col == source * 8 + (row - source * 6))


def pack_kernel(tp_ref, wide_ref, narrow_ref, rope_ref, lat_ref, gain_ref, res_ref, ids_ref, w_ref, cos_ref, sin_ref, out_ref, sel_ref):
    t = tp_ref[0]
    src, dst = iota((16, 128), 0), iota((16, 128), 1)
    turning = (dst < 32) | (dst >= 96)
    spread = jnp.where(turning & ((dst & 15) == src), 1.0, 0.0)
    cos = exact_tn(cos_ref[...], spread) + jnp.where((iota((TOK, 128), 1) >= 32) & (iota((TOK, 128), 1) < 96), 1.0, 0.0)
    sin = exact_tn(sin_ref[...], jnp.where((dst & 16) == 0, -spread, spread))
    src, dst = iota((128, 128), 0), iota((128, 128), 1)
    swap = picks(src == dst + jnp.where((dst & 16) == 0, 16, -16))

    def turned(block):
        return (block.astype(F32) * cos + dot(block, swap) * sin).astype(BF)

    first, after = picks(src == dst), picks(src + 32 == dst)
    q_rest = turned((dot(wide_ref[:, 128:], first[:32]) + dot(narrow_ref[...], after[:96])).astype(BF))
    rope = turned(dot_tn(rope_ref[...], first[:32]).astype(BF))
    lat = lat_ref[...].astype(F32)
    scaled = lat * lax.rsqrt(jnp.mean(lat * lat, axis=1, keepdims=True) + EPS)
    normed = (scaled * gain_ref[...]).astype(BF)
    res = res_ref[:, pl.ds(pl.multiple_of(t * 128, 128), 128)]

    before = picks(iota((TOK, TOK), 0) < iota((TOK, TOK), 1))
    named = [jnp.where(ids_ref[k : k + 1, :] == iota((TOK, TOK), 0), 1.0, 0.0) for k in range(2)]
    rank = dot((named[0] + named[1]).astype(BF), before)
    row, tok = iota((256, TOK), 0), iota((256, TOK), 1)
    dest, place = row >> 3, row & 7
    selects, high, low = [], 0.0, 0.0
    for k in range(2):
        slot = ids_ref[k : k + 1, :] * 3 + jnp.sum(named[k] * rank, axis=0, keepdims=True).astype(jnp.int32)
        mask = (slot == dest * 6 + place) & (place < 6)
        selects.append(picks(mask))
        w = w_ref[k : k + 1, :]
        w_hi = w.astype(BF).astype(F32)
        high = high + jnp.where(mask, w_hi, 0.0)
        low = low + jnp.where(mask, w - w_hi, 0.0)
    either = selects[0] + selects[1]
    sel_ref[...] = either
    start = (dest & 1) * 32 + t * 2
    token_row = picks((place >= 6) & (tok == start + place - 6))
    rope_row = picks((place < 2) & (tok == start + place))
    lat_part = dot(token_row, normed)
    out_ref[:, :128] = (dot(either, wide_ref[:, :128]) + lat_part[:, :128]).astype(BF)
    out_ref[:, 128:256] = (dot(either, q_rest) + lat_part[:, 128:256]).astype(BF)
    out_ref[:, 256:384] = (dot(either, res) + lat_part[:, 256:384]).astype(BF)
    lane, token = iota((TOK, 128), 1), iota((TOK, 128), 0).astype(F32)
    side = dot(either, jnp.where(lane == LANE_POS, token, 0.0).astype(BF))
    side = side + dot(high.astype(BF), picks(lane == LANE_HI)) + dot(low.astype(BF), picks(lane == LANE_LO))
    side = side + dot(selects[0], picks(lane == LANE_FLAG)) + dot(rope_row, rope)
    out_ref[:, 384:] = (side + lat_part[:, 384:]).astype(BF)


def slots_kernel(arr_ref, out_ref):
    out_ref[...] = dot(slot_rows(), arr_ref[...]).astype(BF)


def spread_kernel(arr_ref, out_ref):
    row, col = iota((TOK, 256), 0), iota((TOK, 256), 1)
    base = (row >> 1) * 8 + (row & 1)
    lat = dot(picks(col == base + 6), arr_ref[...]).astype(BF)
    side = arr_ref[:, 384:]
    packed = jnp.zeros((16, 128), F32)
    for b in range(4):
        near, far = iota((16, 256), 0) + 16 * b, iota((16, 256), 1)
        here = dot(picks(far == (near >> 1) * 8 + (near & 1)), side).astype(BF)
        src, dst = iota((128, 128), 0), iota((128, 128), 1)
        packed = packed + dot(here, picks((src < 32) & (dst == src + 32 * b)))
    packed = packed.astype(BF)
    for copy in range(N_TP):
        for f in range(4):
            out_ref[copy, f * TOK : (f + 1) * TOK, :] = lat[:, f * 128 : (f + 1) * 128]
        out_ref[copy, 4 * TOK :, :] = packed


def keys_kernel(lat_ref, wide_ref, narrow_ref, out_ref):
    rows = N_TP * TOK
    wide = jnp.zeros((rows, 256), F32)
    narrow = jnp.zeros((rows, 128), F32)
    for f in range(4):
        part = lat_ref[:, f * TOK : (f + 1) * TOK, :].reshape(rows, 128)
        wide = wide + dot(part, wide_ref[f * 128 : (f + 1) * 128, :])
        narrow = narrow + dot(part, narrow_ref[f * 128 : (f + 1) * 128, :])
    wide, narrow = wide.astype(BF), narrow.astype(BF)
    packed = lat_ref[:, 4 * TOK :, :].reshape(256, 128)
    src, dst = iota((128, 128), 0), iota((128, 128), 1)
    pieces = []
    for b in range(4):
        moved = dot(packed, picks((dst >= 96) & (src == dst - 96 + 32 * b)))
        pieces.append(moved.astype(BF).reshape(N_TP, 16, 128))
    rope = jnp.concatenate(pieces, axis=1).reshape(rows, 128)
    out_ref[0] = wide[:, :128]
    out_ref[1] = wide[:, 128:]
    shifted = dot(narrow, picks((src < 64) & (dst == src + 32)))
    out_ref[2] = (shifted + rope.astype(F32)).astype(BF)
    out_ref[3] = dot(narrow, picks((src >= 64) & (dst == src - 64))).astype(BF)


def half_attention(half, slot_ref, kv_ref):
    q = slot_ref[:, :256]
    side = slot_ref[:, 384:].astype(F32)
    row_pos = div6(iota((SLOTS, 1), 0)) * TOK + lane_value(side, LANE_POS).astype(jnp.int32)
    src, dst = iota((128, 128), 0), iota((128, 128), 1)
    q_rest = q[:, 128:]
    wide_q = jnp.concatenate([q[:, :128], dot(q_rest, picks((src < 32) & (dst == src + 96))).astype(BF)], axis=1)
    narrow_q = jnp.where(iota((SLOTS, 128), 1) >= 32, q_rest.astype(F32), 0.0).astype(BF)
    n = iota((1, N_TP * TOK), 1)
    allowed = ((n & 63) >> 1) * TOK + (n >> 6) * 2 + (n & 1) + half * 32 <= row_pos
    wide = dot_nt(wide_q, jnp.concatenate([kv_ref[0], kv_ref[2]], axis=1)) * (160 ** -0.5)
    narrow = dot_nt(narrow_q, kv_ref[2]) * (96 ** -0.5)
    return [jnp.where(allowed, s, FLOOR) for s in (wide, narrow)]


def weighed(scores, peak, values):
    e = jnp.exp(scores - peak)
    return jnp.sum(e, axis=1, keepdims=True), dot(e.astype(BF), values)


def attend_own_kernel(core_ref, slot_ref, kv_ref, peak_ref, total_ref, sum_ref):
    for i, scores in enumerate(half_attention(core_ref[0], slot_ref, kv_ref)):
        peak = jnp.max(scores, axis=1, keepdims=True)
        total, summed = weighed(scores, peak, kv_ref[1 + 2 * i])
        peak_ref[i] = jnp.broadcast_to(peak, (SLOTS, 128))
        total_ref[i] = jnp.broadcast_to(total, (SLOTS, 128))
        sum_ref[i] = summed


def attend_rest_kernel(core_ref, slot_ref, kv_ref, peak_ref, total_ref, sum_ref, wide_out_ref, narrow_out_ref, out_ref):
    attended = []
    for i, scores in enumerate(half_attention(1 - core_ref[0], slot_ref, kv_ref)):
        old = peak_ref[i][:, :1]
        peak = jnp.maximum(old, jnp.max(scores, axis=1, keepdims=True))
        total, summed = weighed(scores, peak, kv_ref[1 + 2 * i])
        kept = jnp.exp(old - peak)
        attended.append(((summed + kept * sum_ref[i]) / (total + kept * total_ref[i][:, :1])).astype(BF))
    wide_att, narrow_att = attended[0], attended[1][:, :64]
    for piece in range(N_TP):
        cols = slice(piece * 128, (piece + 1) * 128)
        out_ref[piece] = (dot(wide_att, wide_out_ref[:, cols]) + dot(narrow_att, narrow_out_ref[:, cols])).astype(BF)


def stream_kernel(part_ref, slot_ref, out_ref):
    total = jnp.zeros((SLOTS, 128), F32)
    for piece in range(N_TP):
        total = total + part_ref[piece].astype(F32)
    stream = (slot_ref[:, 256:384].astype(F32) + total.astype(BF).astype(F32)).astype(BF)
    for copy in range(N_TP):
        out_ref[copy] = stream


def expert_kernel(x_ref, slot_ref, gain_ref, eg_ref, eu_ref, ed_ref, sg_ref, su_ref, sd_ref, out_ref):
    squares = jnp.zeros((SLOTS, 128), F32)
    for piece in range(N_TP):
        x = x_ref[piece].astype(F32)
        squares = squares + x * x
    scale = lax.rsqrt(jnp.sum(squares, axis=1, keepdims=True) * (1.0 / D_MODEL) + EPS)
    into = jnp.zeros((SLOTS, 384), F32)
    for pair in range(N_TP // 2):
        cols = slice(pair * 256, (pair + 1) * 256)
        x = jnp.concatenate([x_ref[2 * pair], x_ref[2 * pair + 1]], axis=1).astype(F32)
        x = (x * scale * gain_ref[:, cols]).astype(BF)
        weights = [eg_ref[0, :, cols], eg_ref[1, :, cols], sg_ref[:, cols], eu_ref[0, :, cols], eu_ref[1, :, cols], su_ref[:, cols]]
        into = into + dot_nt(x, jnp.concatenate(weights, axis=0))
    gate, up = into[:, :192], into[:, 192:]
    hidden = (gate / (1.0 + jnp.exp(-gate))) * up
    side = slot_ref[:, 384:].astype(F32)
    weight = lane_value(side, LANE_HI) + lane_value(side, LANE_LO)
    flag = lane_value(side, LANE_FLAG)
    owner = div3(iota((SLOTS, 128), 0)) & 1
    routed_hidden = jnp.where(owner == (iota((SLOTS, 128), 1) >> 6), hidden[:, :128], 0.0).astype(BF)
    shared_hidden = hidden[:, 128:].astype(BF)
    for piece in range(N_TP // 2):
        cols = slice(piece * 256, (piece + 1) * 256)
        routed = dot(routed_hidden, ed_ref[:, cols])
        shared = dot(shared_hidden, sd_ref[:, cols])
        both = (weight * routed + flag * shared).astype(BF)
        out_ref[2 * piece] = both[:, :128]
        out_ref[2 * piece + 1] = both[:, 128:]


def give_back_kernel(part_ref, stream_ref, slot_ref, out_ref):
    total = jnp.zeros((SLOTS, 128), F32)
    for piece in range(N_TP):
        total = total + part_ref[piece].astype(F32)
    flag = lane_value(slot_ref[:, 384:].astype(F32), LANE_FLAG)
    total = (total + flag * stream_ref[0].astype(F32)).astype(BF)
    out_ref[...] = dot_tn(slot_rows(), total).astype(BF)


def finish_kernel(sel_ref, back_ref, out_ref):
    out_ref[...] = dot_tn(sel_ref[...], back_ref[...]).astype(BF)


VMEM = pl.BlockSpec(memory_space=pltpu.VMEM)
SMEM = pl.BlockSpec(memory_space=pltpu.SMEM)


def run(kernel, outs, *args, scalars=0, plain=0, spread=True, kind=BF):
    spaces = [pltpu.HBM if i < plain else pltpu.VMEM for i in range(scalars, len(args))]
    placed = [pltpu.with_memory_space_constraint(a, m) for a, m in zip(args[scalars:], spaces)]
    args = [*args[:scalars], *placed]
    return pl.pallas_call(
        kernel,
        out_shape=[pltpu.VMEM(shape, kind) for shape in outs] if spread else jax.ShapeDtypeStruct(outs[0], BF),
        in_specs=[SMEM] * scalars + [VMEM] * (len(args) - scalars),
        out_specs=[VMEM] * len(outs) if spread else VMEM,
        compiler_params=pltpu.CompilerParams(vmem_limit_bytes=24 << 20),
        name=kernel.__name__,
    )(*args)


def swap_all(values, axes):
    return lax.all_to_all(values, axes, split_axis=0, concat_axis=0, tiled=True)


def local(
    wide_queries,
    narrow_queries,
    kv_latent,
    rope_key,
    latent_gain,
    wide_kv_weight,
    narrow_kv_weight,
    wide_out_weight,
    narrow_out_weight,
    residual,
    norm_gain,
    route_ids,
    route_weights,
    expert_gate,
    expert_up,
    expert_down,
    shared_gate,
    shared_up,
    shared_down,
):
    t = lax.axis_index("tp").astype(jnp.int32)[None]
    core = lax.axis_index("c").astype(jnp.int32)[None]
    frequency = THETA ** (-2.0 * jnp.arange(16, dtype=F32) / 32)
    positions = lax.axis_index(SP) * TOK + jnp.arange(TOK, dtype=jnp.int32)
    angles = frequency[:, None] * positions.astype(F32)[None, :]
    payload, chosen = run(
        pack_kernel, [(256, 512), (256, TOK)],
        t, wide_queries, narrow_queries, rope_key.T, kv_latent, latent_gain[None, :], residual,
        route_ids.T, route_weights.T, jnp.cos(angles), jnp.sin(angles),
        scalars=1,
        plain=9,
    )
    arrived = swap_all(payload.reshape(N_SP, 8, 512), SP).reshape(256, 512)
    (spread,) = run(spread_kernel, [(N_TP, 272, 128)], arrived)
    latents = swap_all(spread, "tp")
    (slots,) = run(slots_kernel, [(SLOTS, 512)], arrived)
    (own,) = run(keys_kernel, [(4, N_TP * TOK, 128)], latents, wide_kv_weight, narrow_kv_weight)
    other = lax.ppermute(own, "c", [(0, 1), (1, 0)])
    state = run(attend_own_kernel, [(2, SLOTS, 128)] * 3, core, slots, own, scalars=1, kind=F32)
    (partial,) = run(
        attend_rest_kernel, [(N_TP, SLOTS, 128)],
        core, slots, other, *state, wide_out_weight, narrow_out_weight,
        scalars=1,
    )
    (copies,) = run(stream_kernel, [(N_TP, SLOTS, 128)], swap_all(partial, "tp"), slots)
    rows = swap_all(copies, "tp")
    (partial,) = run(
        expert_kernel, [(N_TP, SLOTS, 128)],
        rows, slots, norm_gain[None, :],
        expert_gate.swapaxes(1, 2), expert_up.swapaxes(1, 2), expert_down.reshape(128, D_MODEL),
        shared_gate.T, shared_up.T, shared_down,
    )
    (back,) = run(give_back_kernel, [(256, 128)], swap_all(partial, "tp"), copies, slots)
    back = swap_all(back.reshape(N_SP, 8, 128), SP).reshape(256, 128)
    return run(finish_kernel, [(TOK, 128)], chosen, back, spread=False)


def solution(mesh):
    torus = Mesh(mesh.devices.reshape(16, 2, mesh.shape["tp"]), ("z", "c", "tp"))
    return jax.shard_map(
        local,
        mesh=torus,
        in_specs=(
            P(SP, "tp"),
            P(SP, "tp"),
            P(SP, None),
            P(SP, None),
            P(),
            P(None, "tp"),
            P(None, "tp"),
            P("tp", None),
            P("tp", None),
            P(SP, None),
            P(),
            P(SP, None),
            P(SP, None),
            P(SP, None, "tp"),
            P(SP, None, "tp"),
            P(SP, "tp", None),
            P(None, "tp"),
            P(None, "tp"),
            P("tp", None),
        ),
        out_specs=P(SP, "tp"),
        check_vma=False,
    )
```

```python
import functools

import jax
import jax.numpy as jnp
from jax import lax
from jax.experimental import pallas as pl
from jax.experimental.pallas import tpu as pltpu
from jax.sharding import Mesh
from jax.sharding import PartitionSpec as P

D_MODEL = 2048
THETA = 10000.0
EPS = 1e-06
FLOOR = -1e30
SP = ("z", "c")
N_SP = 32
N_TP = 16
TOK = 64
SLOTS = 192
F32 = jnp.float32
BF = jnp.bfloat16

ROWS = 28
LANE_POS, LANE_HI, LANE_LO, LANE_FLAG = 64, 65, 66, 67


def iota(shape, dim):
    return lax.broadcasted_iota(jnp.int32, shape, dim)


def div6(v):
    return (v * 10923) >> 16


def div3(v):
    return (v * 21846) >> 16


def div28(v):
    return (v * 2341) >> 16


def dot(a, b):
    return jnp.dot(a, b, preferred_element_type=F32)


def dot_nt(a, b):
    return lax.dot_general(a, b, (((1,), (1,)), ((), ())), preferred_element_type=F32)


def dot_tn(a, b):
    return lax.dot_general(a, b, (((0,), (0,)), ((), ())), preferred_element_type=F32)


def exact_tn(a, b):
    return lax.dot_general(
        a, b, (((0,), (0,)), ((), ())), precision=lax.Precision.HIGHEST, preferred_element_type=F32
    )


def picks(mask):
    return jnp.where(mask, 1.0, 0.0).astype(BF)


def side_value(block, lane):
    row = iota((SLOTS, 1), 0)
    return jnp.sum(jnp.where(iota(block.shape, 1) == lane + 4 * (row - 3 * div3(row)), block, 0.0), axis=1, keepdims=True)


def from_rows(source, row):
    count = source.shape[0]
    return picks(iota((count, N_SP * ROWS), 1) == source * ROWS + row)


def pack_kernel(tp_ref, wide_ref, narrow_ref, rope_ref, lat_ref, gain_ref, res_ref, ids_ref, w_ref, cos_ref, sin_ref, out_ref, sel_ref):
    t = tp_ref[0]
    src, dst = iota((16, 128), 0), iota((16, 128), 1)
    turning = (dst < 32) | (dst >= 96)
    spread = jnp.where(turning & ((dst & 15) == src), 1.0, 0.0)
    cos = exact_tn(cos_ref[...], spread) + jnp.where((iota((TOK, 128), 1) >= 32) & (iota((TOK, 128), 1) < 96), 1.0, 0.0)
    sin = exact_tn(sin_ref[...], jnp.where((dst & 16) == 0, -spread, spread))
    src, dst = iota((128, 128), 0), iota((128, 128), 1)
    swap = picks(src == dst + jnp.where((dst & 16) == 0, 16, -16))

    def turned(block):
        return (block.astype(F32) * cos + dot(block, swap) * sin).astype(BF)

    first, after = picks(src == dst), picks(src + 32 == dst)
    q_rest = turned((dot(wide_ref[:, 128:], first[:32]) + dot(narrow_ref[...], after[:96])).astype(BF))
    rope = turned(dot_tn(rope_ref[...], first[:32]).astype(BF))
    lat = lat_ref[...].astype(F32)
    scaled = lat * lax.rsqrt(jnp.mean(lat * lat, axis=1, keepdims=True) + EPS)
    normed = (scaled * gain_ref[...]).astype(BF)
    res = res_ref[:, pl.ds(pl.multiple_of(t * 128, 128), 128)]

    before = picks(iota((TOK, TOK), 0) < iota((TOK, TOK), 1))
    named = [jnp.where(ids_ref[k : k + 1, :] == iota((TOK, TOK), 0), 1.0, 0.0) for k in range(2)]
    rank = dot((named[0] + named[1]).astype(BF), before)
    slots = [
        ids_ref[k : k + 1, :] * 3 + jnp.sum(named[k] * rank, axis=0, keepdims=True).astype(jnp.int32) for k in range(2)
    ]

    def either(want):
        return picks((slots[0] == want) | (slots[1] == want))

    sel_ref[...] = either(iota((SLOTS, 1), 0))

    row = iota((TOK, 1), 0)
    lane, token = iota((TOK, 128), 1), iota((TOK, 128), 0).astype(F32)
    side = dot(picks(iota((TOK, TOK), 1) == ((row >> 1) & 1) * 32 + t * 2 + (row & 1)), rope)
    for place in range(3):
        high, low, flag = 0.0, 0.0, 0.0
        for k in range(2):
            mask = slots[k] == row * 3 + place
            w = w_ref[k : k + 1, :]
            w_hi = w.astype(BF).astype(F32)
            high = high + jnp.where(mask, w_hi, 0.0)
            low = low + jnp.where(mask, w - w_hi, 0.0)
            flag = flag + jnp.where(mask, 1.0 - k, 0.0)
        at = lane - 4 * place
        side = side + dot(either(row * 3 + place), jnp.where(at == LANE_POS, token, 0.0).astype(BF))
        side = side + dot(high.astype(BF), picks(at == LANE_HI)) + dot(low.astype(BF), picks(at == LANE_LO))
        side = side + dot(flag.astype(BF), picks(at == LANE_FLAG))

    row = iota((N_SP * ROWS, 1), 0)
    dest = div28(row)
    place = row - dest * ROWS
    kind = div6(place)
    slot = dest * 6 + place - kind * 6
    out = 0.0
    for i, rows in enumerate((wide_ref[:, :128], q_rest, res)):
        out = out + dot(either(jnp.where(kind == i, slot, -1)), rows)
    start = (dest & 1) * 32 + t * 2
    tok = iota((N_SP * ROWS, TOK), 1)
    for f in range(4):
        mine = (place >> 1) == 9 + f
        out = out + dot(picks(tok == jnp.where(mine, start + (place & 1), -1)), normed[:, f * 128 : (f + 1) * 128])
    out = out + dot(picks(tok == jnp.where(place >= 26, dest * 2 + place - 26, -1)), side.astype(BF))
    out_ref[...] = out.astype(BF)


def slots_kernel(arr_ref, out_ref):
    row = iota((SLOTS, 1), 0)
    source = div6(row)
    place = row - source * 6
    for i, start in enumerate((place, place + 6, place + 12, 26 + div3(place))):
        out_ref[:, i * 128 : (i + 1) * 128] = dot(from_rows(source, start), arr_ref[...]).astype(BF)


def spread_kernel(arr_ref, out_ref):
    n = iota((TOK, 1), 0)
    rows = [dot(from_rows(n >> 1, 18 + 2 * f + (n & 1)), arr_ref[...]).astype(BF) for f in range(4)]
    rope = dot(from_rows(n >> 1, 26 + (n & 1)), arr_ref[...]).astype(BF)
    packed = jnp.zeros((16, 128), F32)
    src, dst = iota((128, 128), 0), iota((128, 128), 1)
    for b in range(4):
        packed = packed + dot(rope[16 * b : 16 * (b + 1)], picks((src < 32) & (dst == src + 32 * b)))
    packed = packed.astype(BF)
    for copy in range(N_TP):
        for f in range(4):
            out_ref[copy, f * TOK : (f + 1) * TOK, :] = rows[f]
        out_ref[copy, 4 * TOK :, :] = packed


def keys_kernel(lat_ref, wide_ref, narrow_ref, out_ref):
    rows = N_TP * TOK
    wide = jnp.zeros((rows, 256), F32)
    narrow = jnp.zeros((rows, 128), F32)
    for f in range(4):
        part = lat_ref[:, f * TOK : (f + 1) * TOK, :].reshape(rows, 128)
        wide = wide + dot(part, wide_ref[f * 128 : (f + 1) * 128, :])
        narrow = narrow + dot(part, narrow_ref[f * 128 : (f + 1) * 128, :])
    wide, narrow = wide.astype(BF), narrow.astype(BF)
    packed = lat_ref[:, 4 * TOK :, :].reshape(256, 128)
    src, dst = iota((128, 128), 0), iota((128, 128), 1)
    pieces = []
    for b in range(4):
        moved = dot(packed, picks((dst >= 96) & (src == dst - 96 + 32 * b)))
        pieces.append(moved.astype(BF).reshape(N_TP, 16, 128))
    rope = jnp.concatenate(pieces, axis=1).reshape(rows, 128)
    out_ref[0] = wide[:, :128]
    out_ref[1] = wide[:, 128:]
    shifted = dot(narrow, picks((src < 64) & (dst == src + 32)))
    out_ref[2] = (shifted + rope.astype(F32)).astype(BF)
    out_ref[3] = dot(narrow, picks((src >= 64) & (dst == src - 64))).astype(BF)


def half_attention(half, slot_ref, kv_ref):
    q = slot_ref[:, :256]
    side = slot_ref[:, 384:].astype(F32)
    row_pos = div6(iota((SLOTS, 1), 0)) * TOK + side_value(side, LANE_POS).astype(jnp.int32)
    src, dst = iota((128, 128), 0), iota((128, 128), 1)
    q_rest = q[:, 128:]
    wide_q = jnp.concatenate([q[:, :128], dot(q_rest, picks((src < 32) & (dst == src + 96))).astype(BF)], axis=1)
    narrow_q = jnp.where(iota((SLOTS, 128), 1) >= 32, q_rest.astype(F32), 0.0).astype(BF)
    n = iota((1, N_TP * TOK), 1)
    allowed = ((n & 63) >> 1) * TOK + (n >> 6) * 2 + (n & 1) + half * 32 <= row_pos
    wide = dot_nt(wide_q, jnp.concatenate([kv_ref[0], kv_ref[2]], axis=1)) * (160 ** -0.5)
    narrow = dot_nt(narrow_q, kv_ref[2]) * (96 ** -0.5)
    return [jnp.where(allowed, s, FLOOR) for s in (wide, narrow)]


def weighed(scores, peak, values):
    e = jnp.exp(scores - peak)
    return jnp.sum(e, axis=1, keepdims=True), dot(e.astype(BF), values)


def attend_own_kernel(core_ref, slot_ref, kv_ref, peak_ref, total_ref, sum_ref):
    for i, scores in enumerate(half_attention(core_ref[0], slot_ref, kv_ref)):
        peak = jnp.max(scores, axis=1, keepdims=True)
        total, summed = weighed(scores, peak, kv_ref[1 + 2 * i])
        peak_ref[i] = jnp.broadcast_to(peak, (SLOTS, 128))
        total_ref[i] = jnp.broadcast_to(total, (SLOTS, 128))
        sum_ref[i] = summed


def attend_rest_kernel(core_ref, slot_ref, kv_ref, peak_ref, total_ref, sum_ref, wide_out_ref, narrow_out_ref, out_ref):
    attended = []
    for i, scores in enumerate(half_attention(1 - core_ref[0], slot_ref, kv_ref)):
        old = peak_ref[i][:, :1]
        peak = jnp.maximum(old, jnp.max(scores, axis=1, keepdims=True))
        total, summed = weighed(scores, peak, kv_ref[1 + 2 * i])
        kept = jnp.exp(old - peak)
        attended.append(((summed + kept * sum_ref[i]) / (total + kept * total_ref[i][:, :1])).astype(BF))
    wide_att, narrow_att = attended[0], attended[1][:, :64]
    for piece in range(N_TP):
        cols = slice(piece * 128, (piece + 1) * 128)
        out_ref[piece] = (dot(wide_att, wide_out_ref[:, cols]) + dot(narrow_att, narrow_out_ref[:, cols])).astype(BF)


def stream_kernel(part_ref, slot_ref, out_ref):
    total = jnp.zeros((SLOTS, 128), F32)
    for piece in range(N_TP):
        total = total + part_ref[piece].astype(F32)
    stream = (slot_ref[:, 256:384].astype(F32) + total.astype(BF).astype(F32)).astype(BF)
    for copy in range(N_TP):
        out_ref[copy] = stream


def expert_kernel(x_ref, slot_ref, gain_ref, eg_ref, eu_ref, ed_ref, sg_ref, su_ref, sd_ref, out_ref):
    squares = jnp.zeros((SLOTS, 128), F32)
    for piece in range(N_TP):
        x = x_ref[piece].astype(F32)
        squares = squares + x * x
    scale = lax.rsqrt(jnp.sum(squares, axis=1, keepdims=True) * (1.0 / D_MODEL) + EPS)
    into = jnp.zeros((SLOTS, 384), F32)
    for pair in range(N_TP // 2):
        cols = slice(pair * 256, (pair + 1) * 256)
        x = jnp.concatenate([x_ref[2 * pair], x_ref[2 * pair + 1]], axis=1).astype(F32)
        x = (x * scale * gain_ref[:, cols]).astype(BF)
        weights = [eg_ref[0, :, cols], eg_ref[1, :, cols], sg_ref[:, cols], eu_ref[0, :, cols], eu_ref[1, :, cols], su_ref[:, cols]]
        into = into + dot_nt(x, jnp.concatenate(weights, axis=0))
    gate, up = into[:, :192], into[:, 192:]
    hidden = (gate / (1.0 + jnp.exp(-gate))) * up
    side = slot_ref[:, 384:].astype(F32)
    weight = side_value(side, LANE_HI) + side_value(side, LANE_LO)
    flag = side_value(side, LANE_FLAG)
    owner = div3(iota((SLOTS, 128), 0)) & 1
    routed_hidden = jnp.where(owner == (iota((SLOTS, 128), 1) >> 6), hidden[:, :128], 0.0).astype(BF)
    shared_hidden = hidden[:, 128:].astype(BF)
    for piece in range(N_TP // 2):
        cols = slice(piece * 256, (piece + 1) * 256)
        routed = dot(routed_hidden, ed_ref[:, cols])
        shared = dot(shared_hidden, sd_ref[:, cols])
        both = (weight * routed + flag * shared).astype(BF)
        out_ref[2 * piece] = both[:, :128]
        out_ref[2 * piece + 1] = both[:, 128:]


def give_back_kernel(part_ref, stream_ref, slot_ref, out_ref):
    total = jnp.zeros((SLOTS, 128), F32)
    for piece in range(N_TP):
        total = total + part_ref[piece].astype(F32)
    flag = side_value(slot_ref[:, 384:].astype(F32), LANE_FLAG)
    out_ref[...] = (total + flag * stream_ref[0].astype(F32)).astype(BF)


def finish_kernel(sel_ref, back_ref, out_ref):
    out_ref[...] = dot_tn(sel_ref[...], back_ref[...]).astype(BF)


VMEM = pl.BlockSpec(memory_space=pltpu.VMEM)
SMEM = pl.BlockSpec(memory_space=pltpu.SMEM)


def run(kernel, outs, *args, scalars=0, plain=0, spread=True, kind=BF):
    spaces = [pltpu.HBM if i < plain else pltpu.VMEM for i in range(scalars, len(args))]
    placed = [pltpu.with_memory_space_constraint(a, m) for a, m in zip(args[scalars:], spaces)]
    args = [*args[:scalars], *placed]
    return pl.pallas_call(
        kernel,
        out_shape=[pltpu.VMEM(shape, kind) for shape in outs] if spread else jax.ShapeDtypeStruct(outs[0], BF),
        in_specs=[SMEM] * scalars + [VMEM] * (len(args) - scalars),
        out_specs=[VMEM] * len(outs) if spread else VMEM,
        compiler_params=pltpu.CompilerParams(vmem_limit_bytes=24 << 20),
        name=kernel.__name__,
    )(*args)


def swap_all(values, axes):
    return lax.all_to_all(values, axes, split_axis=0, concat_axis=0, tiled=True)


def local(
    wide_queries,
    narrow_queries,
    kv_latent,
    rope_key,
    latent_gain,
    wide_kv_weight,
    narrow_kv_weight,
    wide_out_weight,
    narrow_out_weight,
    residual,
    norm_gain,
    route_ids,
    route_weights,
    expert_gate,
    expert_up,
    expert_down,
    shared_gate,
    shared_up,
    shared_down,
):
    t = lax.axis_index("tp").astype(jnp.int32)[None]
    core = lax.axis_index("c").astype(jnp.int32)[None]
    frequency = THETA ** (-2.0 * jnp.arange(16, dtype=F32) / 32)
    positions = lax.axis_index(SP) * TOK + jnp.arange(TOK, dtype=jnp.int32)
    angles = frequency[:, None] * positions.astype(F32)[None, :]
    payload, chosen = run(
        pack_kernel, [(N_SP * ROWS, 128), (SLOTS, TOK)],
        t, wide_queries, narrow_queries, rope_key.T, kv_latent, latent_gain[None, :], residual,
        route_ids.T, route_weights.T, jnp.cos(angles), jnp.sin(angles),
        scalars=1,
        plain=9,
    )
    arrived = swap_all(payload.reshape(N_SP, ROWS // 2, 2, 128), SP).reshape(N_SP * ROWS, 128)
    (spread,) = run(spread_kernel, [(N_TP, 272, 128)], arrived)
    latents = swap_all(spread, "tp")
    (slots,) = run(slots_kernel, [(SLOTS, 512)], arrived)
    (own,) = run(keys_kernel, [(4, N_TP * TOK, 128)], latents, wide_kv_weight, narrow_kv_weight)
    other = lax.ppermute(own, "c", [(0, 1), (1, 0)])
    state = run(attend_own_kernel, [(2, SLOTS, 128)] * 3, core, slots, own, scalars=1, kind=F32)
    (partial,) = run(
        attend_rest_kernel, [(N_TP, SLOTS, 128)],
        core, slots, other, *state, wide_out_weight, narrow_out_weight,
        scalars=1,
    )
    (copies,) = run(stream_kernel, [(N_TP, SLOTS, 128)], swap_all(partial, "tp"), slots)
    rows = swap_all(copies, "tp")
    (partial,) = run(
        expert_kernel, [(N_TP, SLOTS, 128)],
        rows, slots, norm_gain[None, :],
        expert_gate.swapaxes(1, 2), expert_up.swapaxes(1, 2), expert_down.reshape(128, D_MODEL),
        shared_gate.T, shared_up.T, shared_down,
    )
    (back,) = run(give_back_kernel, [(SLOTS, 128)], swap_all(partial, "tp"), copies, slots)
    back = swap_all(back.reshape(N_SP, 3, 2, 128), SP).reshape(SLOTS, 128)
    return run(finish_kernel, [(TOK, 128)], chosen, back, spread=False)


def solution(mesh):
    torus = Mesh(mesh.devices.reshape(16, 2, mesh.shape["tp"]), ("z", "c", "tp"))
    return jax.shard_map(
        local,
        mesh=torus,
        in_specs=(
            P(SP, "tp"),
            P(SP, "tp"),
            P(SP, None),
            P(SP, None),
            P(),
            P(None, "tp"),
            P(None, "tp"),
            P("tp", None),
            P("tp", None),
            P(SP, None),
            P(),
            P(SP, None),
            P(SP, None),
            P(SP, None, "tp"),
            P(SP, None, "tp"),
            P(SP, "tp", None),
            P(None, "tp"),
            P(None, "tp"),
            P("tp", None),
        ),
        out_specs=P(SP, "tp"),
        check_vma=False,
    )
```

```python
import functools

import jax
import jax.numpy as jnp
from jax import lax
from jax.experimental import pallas as pl
from jax.experimental.pallas import tpu as pltpu
from jax.sharding import Mesh
from jax.sharding import PartitionSpec as P

D_MODEL = 2048
THETA = 10000.0
EPS = 1e-06
FLOOR = -1e30
SP = ("z", "c")
N_SP = 32
N_TP = 16
TOK = 64
SLOTS = 192
F32 = jnp.float32
BF = jnp.bfloat16

ROWS = 28
LANE_POS, LANE_HI, LANE_LO, LANE_FLAG = 64, 65, 66, 67


def iota(shape, dim):
    return lax.broadcasted_iota(jnp.int32, shape, dim)


def div6(v):
    return (v * 10923) >> 16


def div3(v):
    return (v * 21846) >> 16


def div28(v):
    return (v * 2341) >> 16


def dot(a, b):
    return jnp.dot(a, b, preferred_element_type=F32)


def dot_nt(a, b):
    return lax.dot_general(a, b, (((1,), (1,)), ((), ())), preferred_element_type=F32)


def dot_tn(a, b):
    return lax.dot_general(a, b, (((0,), (0,)), ((), ())), preferred_element_type=F32)


def exact_tn(a, b):
    return lax.dot_general(
        a, b, (((0,), (0,)), ((), ())), precision=lax.Precision.HIGHEST, preferred_element_type=F32
    )


def picks(mask):
    return jnp.where(mask, 1.0, 0.0).astype(BF)


def side_value(block, lane):
    row = iota((SLOTS, 1), 0)
    return jnp.sum(jnp.where(iota(block.shape, 1) == lane + 4 * (row - 3 * div3(row)), block, 0.0), axis=1, keepdims=True)


def from_rows(source, row):
    count = source.shape[0]
    return picks(iota((count, N_SP * ROWS), 1) == source * ROWS + row)


def pack_kernel(tp_ref, wide_ref, narrow_ref, rope_ref, lat_ref, gain_ref, res_ref, ids_ref, w_ref, cos_ref, sin_ref, out_ref, sel_ref):
    t = tp_ref[0]
    src, dst = iota((16, 128), 0), iota((16, 128), 1)
    turning = (dst < 32) | (dst >= 96)
    spread = jnp.where(turning & ((dst & 15) == src), 1.0, 0.0)
    cos = exact_tn(cos_ref[...], spread) + jnp.where((iota((TOK, 128), 1) >= 32) & (iota((TOK, 128), 1) < 96), 1.0, 0.0)
    sin = exact_tn(sin_ref[...], jnp.where((dst & 16) == 0, -spread, spread))
    src, dst = iota((128, 128), 0), iota((128, 128), 1)
    swap = picks(src == dst + jnp.where((dst & 16) == 0, 16, -16))

    def turned(block):
        return (block.astype(F32) * cos + dot(block, swap) * sin).astype(BF)

    first, after = picks(src == dst), picks(src + 32 == dst)
    q_rest = turned((dot(wide_ref[:, 128:], first[:32]) + dot(narrow_ref[...], after[:96])).astype(BF))
    rope = turned(dot_tn(rope_ref[...], first[:32]).astype(BF))
    lat = lat_ref[...].astype(F32)
    scaled = lat * lax.rsqrt(jnp.mean(lat * lat, axis=1, keepdims=True) + EPS)
    normed = (scaled * gain_ref[...]).astype(BF)
    res = res_ref[:, pl.ds(pl.multiple_of(t * 128, 128), 128)]

    before = picks(iota((TOK, TOK), 0) < iota((TOK, TOK), 1))
    named = [jnp.where(ids_ref[k : k + 1, :] == iota((TOK, TOK), 0), 1.0, 0.0) for k in range(2)]
    rank = dot((named[0] + named[1]).astype(BF), before)
    slots = [
        ids_ref[k : k + 1, :] * 3 + jnp.sum(named[k] * rank, axis=0, keepdims=True).astype(jnp.int32) for k in range(2)
    ]

    def either(want):
        return picks((slots[0] == want) | (slots[1] == want))

    sel_ref[...] = either(iota((SLOTS, 1), 0))

    row = iota((TOK, 1), 0)
    lane, token = iota((TOK, 128), 1), iota((TOK, 128), 0).astype(F32)
    side = dot(picks(iota((TOK, TOK), 1) == ((row >> 1) & 1) * 32 + t * 2 + (row & 1)), rope)
    for place in range(3):
        high, low, flag = 0.0, 0.0, 0.0
        for k in range(2):
            mask = slots[k] == row * 3 + place
            w = w_ref[k : k + 1, :]
            w_hi = w.astype(BF).astype(F32)
            high = high + jnp.where(mask, w_hi, 0.0)
            low = low + jnp.where(mask, w - w_hi, 0.0)
            flag = flag + jnp.where(mask, 1.0 - k, 0.0)
        at = lane - 4 * place
        side = side + dot(either(row * 3 + place), jnp.where(at == LANE_POS, token, 0.0).astype(BF))
        side = side + dot(high.astype(BF), picks(at == LANE_HI)) + dot(low.astype(BF), picks(at == LANE_LO))
        side = side + dot(flag.astype(BF), picks(at == LANE_FLAG))

    twice = picks((iota((TOK, 128), 1) & 63) == iota((TOK, 128), 0))
    keys = [dot(slot.astype(F32).astype(BF), twice).astype(jnp.int32) for slot in slots]
    row = iota((N_SP * ROWS, 1), 0)
    dest = div28(row)
    place = row - dest * ROWS
    kind = div6(place)
    slot = dest * 6 + place - kind * 6
    lanes = iota((1, 128), 1)
    tok, upper = lanes & 63, lanes >= 64
    marks = [jnp.where(upper, key + 1024, key) for key in keys]
    want = jnp.where(kind < 2, slot + kind * 1024, -1)
    out = dot(picks((marks[0] == want) | (marks[1] == want)), jnp.concatenate([wide_ref[:, :128], q_rest], axis=0))
    marks = [jnp.where(upper, tok + 1024, key) for key in keys]
    want = jnp.where(kind == 2, slot, jnp.where(place >= 26, dest * 2 + place - 26 + 1024, -1))
    out = out + dot(picks((marks[0] == want) | (marks[1] == want)), jnp.concatenate([res, side.astype(BF)], axis=0))
    start = (dest & 1) * 32 + t * 2 + (place & 1)
    block = (place >> 1) - 9
    for pair in range(2):
        want = jnp.where((block >> 1) == pair, start + (block & 1) * 64, -1)
        rows = [normed[:, f * 128 : (f + 1) * 128] for f in (2 * pair, 2 * pair + 1)]
        out = out + dot(picks(lanes == want), jnp.concatenate(rows, axis=0))
    out_ref[...] = out.astype(BF)


def slots_kernel(arr_ref, out_ref):
    row = iota((SLOTS, 1), 0)
    source = div6(row)
    place = row - source * 6
    for i, start in enumerate((place, place + 6, place + 12, 26 + div3(place))):
        out_ref[:, i * 128 : (i + 1) * 128] = dot(from_rows(source, start), arr_ref[...]).astype(BF)


def spread_kernel(arr_ref, out_ref):
    n = iota((TOK, 1), 0)
    rows = [dot(from_rows(n >> 1, 18 + 2 * f + (n & 1)), arr_ref[...]).astype(BF) for f in range(4)]
    rope = dot(from_rows(n >> 1, 26 + (n & 1)), arr_ref[...]).astype(BF)
    packed = jnp.zeros((16, 128), F32)
    src, dst = iota((128, 128), 0), iota((128, 128), 1)
    for b in range(4):
        packed = packed + dot(rope[16 * b : 16 * (b + 1)], picks((src < 32) & (dst == src + 32 * b)))
    packed = packed.astype(BF)
    for copy in range(N_TP):
        for f in range(4):
            out_ref[copy, f * TOK : (f + 1) * TOK, :] = rows[f]
        out_ref[copy, 4 * TOK :, :] = packed


def keys_kernel(lat_ref, wide_ref, narrow_ref, out_ref):
    rows = N_TP * TOK
    wide = jnp.zeros((rows, 256), F32)
    narrow = jnp.zeros((rows, 128), F32)
    for pair in range(2):
        parts = [lat_ref[:, f * TOK : (f + 1) * TOK, :].reshape(rows, 128) for f in (2 * pair, 2 * pair + 1)]
        part = jnp.concatenate(parts, axis=1)
        wide = wide + dot(part, wide_ref[pair * 256 : (pair + 1) * 256, :])
        narrow = narrow + dot(part, narrow_ref[pair * 256 : (pair + 1) * 256, :])
    wide, narrow = wide.astype(BF), narrow.astype(BF)
    packed = lat_ref[:, 4 * TOK :, :].reshape(256, 128)
    src, dst = iota((128, 128), 0), iota((128, 128), 1)
    pieces = []
    for b in range(4):
        moved = dot(packed, picks((dst >= 96) & (src == dst - 96 + 32 * b)))
        pieces.append(moved.astype(BF).reshape(N_TP, 16, 128))
    rope = jnp.concatenate(pieces, axis=1).reshape(rows, 128)
    out_ref[0] = wide[:, :128]
    out_ref[1] = wide[:, 128:]
    shifted = dot(narrow, picks((src < 64) & (dst == src + 32)))
    out_ref[2] = (shifted + rope.astype(F32)).astype(BF)
    out_ref[3] = dot(narrow, picks((src >= 64) & (dst == src - 64))).astype(BF)


def half_attention(half, slot_ref, kv_ref):
    q = slot_ref[:, :256]
    side = slot_ref[:, 384:].astype(F32)
    row_pos = div6(iota((SLOTS, 1), 0)) * TOK + side_value(side, LANE_POS).astype(jnp.int32)
    src, dst = iota((128, 128), 0), iota((128, 128), 1)
    q_rest = q[:, 128:]
    wide_q = jnp.concatenate([q[:, :128], dot(q_rest, picks((src < 32) & (dst == src + 96))).astype(BF)], axis=1)
    narrow_q = jnp.where(iota((SLOTS, 128), 1) >= 32, q_rest.astype(F32), 0.0).astype(BF)
    n = iota((1, N_TP * TOK), 1)
    allowed = ((n & 63) >> 1) * TOK + (n >> 6) * 2 + (n & 1) + half * 32 <= row_pos
    wide = dot_nt(wide_q, jnp.concatenate([kv_ref[0], kv_ref[2]], axis=1)) * (160 ** -0.5)
    narrow = dot_nt(narrow_q, kv_ref[2]) * (96 ** -0.5)
    return [jnp.where(allowed, s, FLOOR) for s in (wide, narrow)]


def weighed(scores, peak, values):
    e = jnp.exp(scores - peak)
    return jnp.sum(e, axis=1, keepdims=True), dot(e.astype(BF), values)


def attend_own_kernel(core_ref, slot_ref, kv_ref, peak_ref, total_ref, sum_ref):
    for i, scores in enumerate(half_attention(core_ref[0], slot_ref, kv_ref)):
        peak = jnp.max(scores, axis=1, keepdims=True)
        total, summed = weighed(scores, peak, kv_ref[1 + 2 * i])
        peak_ref[i] = jnp.broadcast_to(peak, (SLOTS, 128))
        total_ref[i] = jnp.broadcast_to(total, (SLOTS, 128))
        sum_ref[i] = summed


def attend_rest_kernel(core_ref, slot_ref, kv_ref, peak_ref, total_ref, sum_ref, wide_out_ref, narrow_out_ref, out_ref):
    attended = []
    for i, scores in enumerate(half_attention(1 - core_ref[0], slot_ref, kv_ref)):
        old = peak_ref[i][:, :1]
        peak = jnp.maximum(old, jnp.max(scores, axis=1, keepdims=True))
        total, summed = weighed(scores, peak, kv_ref[1 + 2 * i])
        kept = jnp.exp(old - peak)
        attended.append(((summed + kept * sum_ref[i]) / (total + kept * total_ref[i][:, :1])).astype(BF))
    wide_att, narrow_att = attended[0], attended[1][:, :64]
    for pair in range(N_TP // 2):
        cols = slice(pair * 256, (pair + 1) * 256)
        both = (dot(wide_att, wide_out_ref[:, cols]) + dot(narrow_att, narrow_out_ref[:, cols])).astype(BF)
        out_ref[2 * pair] = both[:, :128]
        out_ref[2 * pair + 1] = both[:, 128:]


def stream_kernel(part_ref, slot_ref, out_ref):
    total = jnp.zeros((SLOTS, 128), F32)
    for piece in range(N_TP):
        total = total + part_ref[piece].astype(F32)
    stream = (slot_ref[:, 256:384].astype(F32) + total.astype(BF).astype(F32)).astype(BF)
    for copy in range(N_TP):
        out_ref[copy] = stream


def expert_kernel(x_ref, slot_ref, gain_ref, eg_ref, eu_ref, ed_ref, sg_ref, su_ref, sd_ref, out_ref):
    squares = jnp.zeros((SLOTS, 128), F32)
    for piece in range(N_TP):
        x = x_ref[piece].astype(F32)
        squares = squares + x * x
    scale = lax.rsqrt(jnp.sum(squares, axis=1, keepdims=True) * (1.0 / D_MODEL) + EPS)
    into = jnp.zeros((SLOTS, 384), F32)
    for pair in range(N_TP // 2):
        cols = slice(pair * 256, (pair + 1) * 256)
        x = jnp.concatenate([x_ref[2 * pair], x_ref[2 * pair + 1]], axis=1).astype(F32)
        x = (x * scale * gain_ref[:, cols]).astype(BF)
        weights = [eg_ref[0, :, cols], eg_ref[1, :, cols], sg_ref[:, cols], eu_ref[0, :, cols], eu_ref[1, :, cols], su_ref[:, cols]]
        into = into + dot_nt(x, jnp.concatenate(weights, axis=0))
    gate, up = into[:, :192], into[:, 192:]
    hidden = (gate / (1.0 + jnp.exp(-gate))) * up
    side = slot_ref[:, 384:].astype(F32)
    weight = side_value(side, LANE_HI) + side_value(side, LANE_LO)
    flag = side_value(side, LANE_FLAG)
    owner = div3(iota((SLOTS, 128), 0)) & 1
    routed_hidden = jnp.where(owner == (iota((SLOTS, 128), 1) >> 6), hidden[:, :128], 0.0).astype(BF)
    shared_hidden = hidden[:, 128:].astype(BF)
    for piece in range(N_TP // 2):
        cols = slice(piece * 256, (piece + 1) * 256)
        routed = dot(routed_hidden, ed_ref[:, cols])
        shared = dot(shared_hidden, sd_ref[:, cols])
        both = (weight * routed + flag * shared).astype(BF)
        out_ref[2 * piece] = both[:, :128]
        out_ref[2 * piece + 1] = both[:, 128:]


def give_back_kernel(part_ref, stream_ref, slot_ref, out_ref):
    total = jnp.zeros((SLOTS, 128), F32)
    for piece in range(N_TP):
        total = total + part_ref[piece].astype(F32)
    flag = side_value(slot_ref[:, 384:].astype(F32), LANE_FLAG)
    out_ref[...] = (total + flag * stream_ref[0].astype(F32)).astype(BF)


def finish_kernel(sel_ref, back_ref, out_ref):
    out_ref[...] = dot_tn(sel_ref[...], back_ref[...]).astype(BF)


VMEM = pl.BlockSpec(memory_space=pltpu.VMEM)
SMEM = pl.BlockSpec(memory_space=pltpu.SMEM)


def run(kernel, outs, *args, scalars=0, plain=0, spread=True, kind=BF):
    spaces = [pltpu.HBM if i < plain else pltpu.VMEM for i in range(scalars, len(args))]
    placed = [pltpu.with_memory_space_constraint(a, m) for a, m in zip(args[scalars:], spaces)]
    args = [*args[:scalars], *placed]
    return pl.pallas_call(
        kernel,
        out_shape=[pltpu.VMEM(shape, kind) for shape in outs] if spread else jax.ShapeDtypeStruct(outs[0], BF),
        in_specs=[SMEM] * scalars + [VMEM] * (len(args) - scalars),
        out_specs=[VMEM] * len(outs) if spread else VMEM,
        compiler_params=pltpu.CompilerParams(vmem_limit_bytes=24 << 20),
        name=kernel.__name__,
    )(*args)


def swap_all(values, axes):
    return lax.all_to_all(values, axes, split_axis=0, concat_axis=0, tiled=True)


def local(
    wide_queries,
    narrow_queries,
    kv_latent,
    rope_key,
    latent_gain,
    wide_kv_weight,
    narrow_kv_weight,
    wide_out_weight,
    narrow_out_weight,
    residual,
    norm_gain,
    route_ids,
    route_weights,
    expert_gate,
    expert_up,
    expert_down,
    shared_gate,
    shared_up,
    shared_down,
):
    t = lax.axis_index("tp").astype(jnp.int32)[None]
    core = lax.axis_index("c").astype(jnp.int32)[None]
    frequency = THETA ** (-2.0 * jnp.arange(16, dtype=F32) / 32)
    positions = lax.axis_index(SP) * TOK + jnp.arange(TOK, dtype=jnp.int32)
    angles = frequency[:, None] * positions.astype(F32)[None, :]
    payload, chosen = run(
        pack_kernel, [(N_SP * ROWS, 128), (SLOTS, TOK)],
        t, wide_queries, narrow_queries, rope_key.T, kv_latent, latent_gain[None, :], residual,
        route_ids.T, route_weights.T, jnp.cos(angles), jnp.sin(angles),
        scalars=1,
        plain=9,
    )
    arrived = swap_all(payload.reshape(N_SP, ROWS // 2, 2, 128), SP).reshape(N_SP * ROWS, 128)
    (spread,) = run(spread_kernel, [(N_TP, 272, 128)], arrived)
    latents = swap_all(spread, "tp")
    (slots,) = run(slots_kernel, [(SLOTS, 512)], arrived)
    (own,) = run(keys_kernel, [(4, N_TP * TOK, 128)], latents, wide_kv_weight, narrow_kv_weight)
    other = lax.ppermute(own, "c", [(0, 1), (1, 0)])
    state = run(attend_own_kernel, [(2, SLOTS, 128)] * 3, core, slots, own, scalars=1, kind=F32)
    (partial,) = run(
        attend_rest_kernel, [(N_TP, SLOTS, 128)],
        core, slots, other, *state, wide_out_weight, narrow_out_weight,
        scalars=1,
    )
    (copies,) = run(stream_kernel, [(N_TP, SLOTS, 128)], swap_all(partial, "tp"), slots)
    rows = swap_all(copies, "tp")
    (partial,) = run(
        expert_kernel, [(N_TP, SLOTS, 128)],
        rows, slots, norm_gain[None, :],
        expert_gate.swapaxes(1, 2), expert_up.swapaxes(1, 2), expert_down.reshape(128, D_MODEL),
        shared_gate.T, shared_up.T, shared_down,
    )
    (back,) = run(give_back_kernel, [(SLOTS, 128)], swap_all(partial, "tp"), copies, slots)
    back = swap_all(back.reshape(N_SP, 3, 2, 128), SP).reshape(SLOTS, 128)
    return run(finish_kernel, [(TOK, 128)], chosen, back, spread=False)


def solution(mesh):
    torus = Mesh(mesh.devices.reshape(16, 2, mesh.shape["tp"]), ("z", "c", "tp"))
    return jax.shard_map(
        local,
        mesh=torus,
        in_specs=(
            P(SP, "tp"),
            P(SP, "tp"),
            P(SP, None),
            P(SP, None),
            P(),
            P(None, "tp"),
            P(None, "tp"),
            P("tp", None),
            P("tp", None),
            P(SP, None),
            P(),
            P(SP, None),
            P(SP, None),
            P(SP, None, "tp"),
            P(SP, None, "tp"),
            P(SP, "tp", None),
            P(None, "tp"),
            P(None, "tp"),
            P("tp", None),
        ),
        out_specs=P(SP, "tp"),
        check_vma=False,
    )
```

```python
import functools

import jax
import jax.numpy as jnp
from jax import lax
from jax.experimental import pallas as pl
from jax.experimental.pallas import tpu as pltpu
from jax.sharding import Mesh
from jax.sharding import PartitionSpec as P

D_MODEL = 2048
THETA = 10000.0
EPS = 1e-06
FLOOR = -1e30
SP = ("z", "c")
N_SP = 32
N_TP = 16
TOK = 64
SLOTS = 192
F32 = jnp.float32
BF = jnp.bfloat16

ROWS = 28
LANE_POS, LANE_HI, LANE_LO, LANE_FLAG = 64, 65, 66, 67


def iota(shape, dim):
    return lax.broadcasted_iota(jnp.int32, shape, dim)


def div6(v):
    return (v * 10923) >> 16


def div3(v):
    return (v * 21846) >> 16


def div28(v):
    return (v * 2341) >> 16


def dot(a, b):
    return jnp.dot(a, b, preferred_element_type=F32)


def dot_nt(a, b):
    return lax.dot_general(a, b, (((1,), (1,)), ((), ())), preferred_element_type=F32)


def dot_tn(a, b):
    return lax.dot_general(a, b, (((0,), (0,)), ((), ())), preferred_element_type=F32)


def exact_tn(a, b):
    return lax.dot_general(
        a, b, (((0,), (0,)), ((), ())), precision=lax.Precision.HIGHEST, preferred_element_type=F32
    )


def picks(mask):
    return jnp.where(mask, 1.0, 0.0).astype(BF)


def side_value(block, lane):
    row = iota((SLOTS, 1), 0)
    return jnp.sum(jnp.where(iota(block.shape, 1) == lane + 4 * (row - 3 * div3(row)), block, 0.0), axis=1, keepdims=True)


def from_rows(source, row):
    count = source.shape[0]
    return picks(iota((count, N_SP * ROWS), 1) == source * ROWS + row)


def pack_kernel(
    tp_ref, wide_hbm, narrow_hbm, rope_hbm, lat_hbm, gain_hbm, res_hbm, ids_hbm, w_hbm, cos_ref, sin_ref, out_ref, sel_ref,
    ids_ref, w_ref, wide_ref, narrow_ref, rope_ref, lat_ref, gain_ref, res_ref, sems,
):
    t = tp_ref[0]
    own_columns = res_hbm.at[:, pl.ds(pl.multiple_of(t * 128, 128), 128)]
    sources = (ids_hbm, w_hbm, wide_hbm, narrow_hbm, rope_hbm, lat_hbm, gain_hbm, own_columns)
    targets = (ids_ref, w_ref, wide_ref, narrow_ref, rope_ref, lat_ref, gain_ref, res_ref)
    copies = [pltpu.make_async_copy(a, b, sems.at[i]) for i, (a, b) in enumerate(zip(sources, targets))]
    for copy in copies:
        copy.start()
    src, dst = iota((16, 128), 0), iota((16, 128), 1)
    turning = (dst < 32) | (dst >= 96)
    spread = jnp.where(turning & ((dst & 15) == src), 1.0, 0.0)
    cos = exact_tn(cos_ref[...], spread) + jnp.where((iota((TOK, 128), 1) >= 32) & (iota((TOK, 128), 1) < 96), 1.0, 0.0)
    sin = exact_tn(sin_ref[...], jnp.where((dst & 16) == 0, -spread, spread))
    src, dst = iota((128, 128), 0), iota((128, 128), 1)
    swap = picks(src == dst + jnp.where((dst & 16) == 0, 16, -16))
    first, after = picks(src == dst), picks(src + 32 == dst)
    twice = picks((iota((TOK, 128), 1) & 63) == iota((TOK, 128), 0))
    row = iota((4 * ROWS, 128), 0)
    dest = div28(row)
    place = row - dest * ROWS
    kind = div6(place)
    slot = dest * 6 + place - kind * 6
    lanes = iota((4 * ROWS, 128), 1)
    start = (dest & 1) * 32 + t * 2 + (place & 1)
    block = (place >> 1) - 9
    want_query = jnp.where(kind < 2, slot + kind * 1024, -100000)
    want_rest = jnp.where(kind == 2, slot, -100000)
    want_side = jnp.where(place >= 26, dest * 2 + place - 26 + 1024, -100000)
    lat_masks = [picks(lanes == jnp.where((block >> 1) == pair, start + (block & 1) * 64, -1)) for pair in range(2)]

    copies[0].wait()
    copies[1].wait()
    before = picks(iota((TOK, TOK), 0) < iota((TOK, TOK), 1))
    named = [jnp.where(ids_ref[k : k + 1, :] == iota((TOK, TOK), 0), 1.0, 0.0) for k in range(2)]
    rank = dot((named[0] + named[1]).astype(BF), before)
    slots = [
        ids_ref[k : k + 1, :] * 3 + jnp.sum(named[k] * rank, axis=0, keepdims=True).astype(jnp.int32) for k in range(2)
    ]

    def either(want):
        return picks((slots[0] == want) | (slots[1] == want))

    sel_ref[...] = either(iota((SLOTS, TOK), 0))
    lane, token = iota((TOK, 128), 1), iota((TOK, 128), 0).astype(F32)
    expert = iota((TOK, TOK), 0)
    side = 0.0
    for third in range(3):
        high, low, flag = 0.0, 0.0, 0.0
        for k in range(2):
            mask = slots[k] == expert * 3 + third
            w = w_ref[k : k + 1, :]
            w_hi = w.astype(BF).astype(F32)
            high = high + jnp.where(mask, w_hi, 0.0)
            low = low + jnp.where(mask, w - w_hi, 0.0)
            flag = flag + jnp.where(mask, 1.0 - k, 0.0)
        at = lane - 4 * third
        side = side + dot(either(expert * 3 + third), jnp.where(at == LANE_POS, token, 0.0).astype(BF))
        side = side + dot(high.astype(BF), picks(at == LANE_HI)) + dot(low.astype(BF), picks(at == LANE_LO))
        side = side + dot(flag.astype(BF), picks(at == LANE_FLAG))
    keys = [dot(slot.astype(F32).astype(BF), twice).astype(jnp.int32) for slot in slots]
    upper = iota((1, 128), 1) >= 64
    query_keys = [jnp.where(upper, key + 1024, key) for key in keys]
    rest_keys = [jnp.where(upper, -1, key) for key in keys]
    side_key = jnp.where(upper, (iota((1, 128), 1) & 63) + 1024, -1)

    for copy in copies[2:]:
        copy.wait()

    def turned(block):
        return (block.astype(F32) * cos + dot(block, swap) * sin).astype(BF)

    q_rest = turned((dot(wide_ref[:, 128:], first[:32]) + dot(narrow_ref[...], after[:96])).astype(BF))
    rope = turned(dot_tn(rope_ref[...], first[:32]).astype(BF))
    lat = lat_ref[...].astype(F32)
    scaled = lat * lax.rsqrt(jnp.mean(lat * lat, axis=1, keepdims=True) + EPS)
    normed = (scaled * gain_ref[...]).astype(BF)
    side = side + dot(picks(iota((TOK, TOK), 1) == ((expert >> 1) & 1) * 32 + t * 2 + (expert & 1)), rope)
    lat_part = 0.0
    for pair in range(2):
        rows = [normed[:, f * 128 : (f + 1) * 128] for f in (2 * pair, 2 * pair + 1)]
        lat_part = lat_part + dot(lat_masks[pair], jnp.concatenate(rows, axis=0))
    query_rows = jnp.concatenate([wide_ref[:, :128], q_rest], axis=0)
    rest_rows = jnp.concatenate([res_ref[...], side.astype(BF)], axis=0)
    for part in range(N_SP // 4):
        want = want_query + 24 * part
        out = dot(picks((query_keys[0] == want) | (query_keys[1] == want)), query_rows)
        want = want_rest + 24 * part
        mask = (rest_keys[0] == want) | (rest_keys[1] == want) | (side_key == want_side + 8 * part)
        out = out + dot(picks(mask), rest_rows)
        out_ref[part * 4 * ROWS : (part + 1) * 4 * ROWS, :] = (out + lat_part).astype(BF)


def slots_kernel(arr_ref, out_ref):
    row = iota((SLOTS, 1), 0)
    source = div6(row)
    place = row - source * 6
    for i, start in enumerate((place, place + 6, place + 12, 26 + div3(place))):
        out_ref[:, i * 128 : (i + 1) * 128] = dot(from_rows(source, start), arr_ref[...]).astype(BF)


def spread_kernel(arr_ref, out_ref):
    n = iota((TOK, 1), 0)
    rows = [dot(from_rows(n >> 1, 18 + 2 * f + (n & 1)), arr_ref[...]).astype(BF) for f in range(4)]
    rope = dot(from_rows(n >> 1, 26 + (n & 1)), arr_ref[...]).astype(BF)
    packed = jnp.zeros((16, 128), F32)
    src, dst = iota((128, 128), 0), iota((128, 128), 1)
    for b in range(4):
        packed = packed + dot(rope[16 * b : 16 * (b + 1)], picks((src < 32) & (dst == src + 32 * b)))
    packed = packed.astype(BF)
    for copy in range(N_TP):
        for f in range(4):
            out_ref[copy, f * TOK : (f + 1) * TOK, :] = rows[f]
        out_ref[copy, 4 * TOK :, :] = packed


def keys_kernel(lat_ref, wide_ref, narrow_ref, out_ref):
    rows = N_TP * TOK
    wide = jnp.zeros((rows, 256), F32)
    narrow = jnp.zeros((rows, 128), F32)
    for pair in range(2):
        parts = [lat_ref[:, f * TOK : (f + 1) * TOK, :].reshape(rows, 128) for f in (2 * pair, 2 * pair + 1)]
        part = jnp.concatenate(parts, axis=1)
        wide = wide + dot(part, wide_ref[pair * 256 : (pair + 1) * 256, :])
        narrow = narrow + dot(part, narrow_ref[pair * 256 : (pair + 1) * 256, :])
    wide, narrow = wide.astype(BF), narrow.astype(BF)
    packed = lat_ref[:, 4 * TOK :, :].reshape(256, 128)
    src, dst = iota((128, 128), 0), iota((128, 128), 1)
    pieces = []
    for b in range(4):
        moved = dot(packed, picks((dst >= 96) & (src == dst - 96 + 32 * b)))
        pieces.append(moved.astype(BF).reshape(N_TP, 16, 128))
    rope = jnp.concatenate(pieces, axis=1).reshape(rows, 128)
    out_ref[0] = wide[:, :128]
    out_ref[1] = wide[:, 128:]
    shifted = dot(narrow, picks((src < 64) & (dst == src + 32)))
    out_ref[2] = (shifted + rope.astype(F32)).astype(BF)
    out_ref[3] = dot(narrow, picks((src >= 64) & (dst == src - 64))).astype(BF)


def half_attention(half, slot_ref, kv_ref):
    q = slot_ref[:, :256]
    side = slot_ref[:, 384:].astype(F32)
    row_pos = div6(iota((SLOTS, 1), 0)) * TOK + side_value(side, LANE_POS).astype(jnp.int32)
    src, dst = iota((128, 128), 0), iota((128, 128), 1)
    q_rest = q[:, 128:]
    wide_q = jnp.concatenate([q[:, :128], dot(q_rest, picks((src < 32) & (dst == src + 96))).astype(BF)], axis=1)
    narrow_q = jnp.where(iota((SLOTS, 128), 1) >= 32, q_rest.astype(F32), 0.0).astype(BF)
    n = iota((1, N_TP * TOK), 1)
    allowed = ((n & 63) >> 1) * TOK + (n >> 6) * 2 + (n & 1) + half * 32 <= row_pos
    wide = dot_nt(wide_q, jnp.concatenate([kv_ref[0], kv_ref[2]], axis=1)) * (160 ** -0.5)
    narrow = dot_nt(narrow_q, kv_ref[2]) * (96 ** -0.5)
    return [jnp.where(allowed, s, FLOOR) for s in (wide, narrow)]


def weighed(scores, peak, values):
    e = jnp.exp(scores - peak)
    return jnp.sum(e, axis=1, keepdims=True), dot(e.astype(BF), values)


def attend_own_kernel(core_ref, slot_ref, kv_ref, peak_ref, total_ref, sum_ref):
    for i, scores in enumerate(half_attention(core_ref[0], slot_ref, kv_ref)):
        peak = jnp.max(scores, axis=1, keepdims=True)
        total, summed = weighed(scores, peak, kv_ref[1 + 2 * i])
        peak_ref[i] = jnp.broadcast_to(peak, (SLOTS, 128))
        total_ref[i] = jnp.broadcast_to(total, (SLOTS, 128))
        sum_ref[i] = summed


def attend_rest_kernel(core_ref, slot_ref, kv_ref, peak_ref, total_ref, sum_ref, wide_out_ref, narrow_out_ref, out_ref):
    attended = []
    for i, scores in enumerate(half_attention(1 - core_ref[0], slot_ref, kv_ref)):
        old = peak_ref[i][:, :1]
        peak = jnp.maximum(old, jnp.max(scores, axis=1, keepdims=True))
        total, summed = weighed(scores, peak, kv_ref[1 + 2 * i])
        kept = jnp.exp(old - peak)
        attended.append(((summed + kept * sum_ref[i]) / (total + kept * total_ref[i][:, :1])).astype(BF))
    wide_att, narrow_att = attended[0], attended[1][:, :64]
    for pair in range(N_TP // 2):
        cols = slice(pair * 256, (pair + 1) * 256)
        both = (dot(wide_att, wide_out_ref[:, cols]) + dot(narrow_att, narrow_out_ref[:, cols])).astype(BF)
        out_ref[2 * pair] = both[:, :128]
        out_ref[2 * pair + 1] = both[:, 128:]


def stream_kernel(part_ref, slot_ref, out_ref):
    total = jnp.zeros((SLOTS, 128), F32)
    for piece in range(N_TP):
        total = total + part_ref[piece].astype(F32)
    stream = (slot_ref[:, 256:384].astype(F32) + total.astype(BF).astype(F32)).astype(BF)
    for copy in range(N_TP):
        out_ref[copy] = stream


def expert_kernel(x_ref, slot_ref, gain_ref, eg_ref, eu_ref, ed_ref, sg_ref, su_ref, sd_ref, out_ref):
    squares = jnp.zeros((SLOTS, 128), F32)
    for piece in range(N_TP):
        x = x_ref[piece].astype(F32)
        squares = squares + x * x
    scale = lax.rsqrt(jnp.sum(squares, axis=1, keepdims=True) * (1.0 / D_MODEL) + EPS)
    into = jnp.zeros((SLOTS, 384), F32)
    for pair in range(N_TP // 2):
        cols = slice(pair * 256, (pair + 1) * 256)
        x = jnp.concatenate([x_ref[2 * pair], x_ref[2 * pair + 1]], axis=1).astype(F32)
        x = (x * scale * gain_ref[:, cols]).astype(BF)
        weights = [eg_ref[0, :, cols], eg_ref[1, :, cols], sg_ref[:, cols], eu_ref[0, :, cols], eu_ref[1, :, cols], su_ref[:, cols]]
        into = into + dot_nt(x, jnp.concatenate(weights, axis=0))
    gate, up = into[:, :192], into[:, 192:]
    hidden = (gate / (1.0 + jnp.exp(-gate))) * up
    side = slot_ref[:, 384:].astype(F32)
    weight = side_value(side, LANE_HI) + side_value(side, LANE_LO)
    flag = side_value(side, LANE_FLAG)
    owner = div3(iota((SLOTS, 128), 0)) & 1
    routed_hidden = jnp.where(owner == (iota((SLOTS, 128), 1) >> 6), hidden[:, :128], 0.0).astype(BF)
    shared_hidden = hidden[:, 128:].astype(BF)
    for piece in range(N_TP // 2):
        cols = slice(piece * 256, (piece + 1) * 256)
        routed = dot(routed_hidden, ed_ref[:, cols])
        shared = dot(shared_hidden, sd_ref[:, cols])
        both = (weight * routed + flag * shared).astype(BF)
        out_ref[2 * piece] = both[:, :128]
        out_ref[2 * piece + 1] = both[:, 128:]


def give_back_kernel(part_ref, stream_ref, slot_ref, out_ref):
    total = jnp.zeros((SLOTS, 128), F32)
    for piece in range(N_TP):
        total = total + part_ref[piece].astype(F32)
    flag = side_value(slot_ref[:, 384:].astype(F32), LANE_FLAG)
    out_ref[...] = (total + flag * stream_ref[0].astype(F32)).astype(BF)


def finish_kernel(sel_ref, back_ref, out_ref):
    out_ref[...] = dot_tn(sel_ref[...], back_ref[...]).astype(BF)


VMEM = pl.BlockSpec(memory_space=pltpu.VMEM)
SMEM = pl.BlockSpec(memory_space=pltpu.SMEM)


HBM = pl.BlockSpec(memory_space=pltpu.HBM)


def run(kernel, outs, *args, scalars=0, plain=0, spread=True, kind=BF, scratch=()):
    spaces = [pltpu.HBM if i < plain else pltpu.VMEM for i in range(scalars, len(args))]
    placed = [pltpu.with_memory_space_constraint(a, m) for a, m in zip(args[scalars:], spaces)]
    args = [*args[:scalars], *placed]
    return pl.pallas_call(
        kernel,
        out_shape=[pltpu.VMEM(shape, kind) for shape in outs] if spread else jax.ShapeDtypeStruct(outs[0], BF),
        in_specs=[SMEM] * scalars + [HBM if m is pltpu.HBM else VMEM for m in spaces],
        out_specs=[VMEM] * len(outs) if spread else VMEM,
        scratch_shapes=scratch,
        compiler_params=pltpu.CompilerParams(vmem_limit_bytes=24 << 20),
        name=kernel.__name__,
    )(*args)


def swap_all(values, axes):
    return lax.all_to_all(values, axes, split_axis=0, concat_axis=0, tiled=True)


def local(
    wide_queries,
    narrow_queries,
    kv_latent,
    rope_key,
    latent_gain,
    wide_kv_weight,
    narrow_kv_weight,
    wide_out_weight,
    narrow_out_weight,
    residual,
    norm_gain,
    route_ids,
    route_weights,
    expert_gate,
    expert_up,
    expert_down,
    shared_gate,
    shared_up,
    shared_down,
):
    t = lax.axis_index("tp").astype(jnp.int32)[None]
    core = lax.axis_index("c").astype(jnp.int32)[None]
    frequency = THETA ** (-2.0 * jnp.arange(16, dtype=F32) / 32)
    positions = lax.axis_index(SP) * TOK + jnp.arange(TOK, dtype=jnp.int32)
    angles = frequency[:, None] * positions.astype(F32)[None, :]
    payload, chosen = run(
        pack_kernel, [(N_SP * ROWS, 128), (SLOTS, TOK)],
        t, wide_queries, narrow_queries, rope_key.T, kv_latent, latent_gain[None, :], residual,
        route_ids.T, route_weights.T, jnp.cos(angles), jnp.sin(angles),
        scalars=1,
        plain=9,
        scratch=[
            pltpu.VMEM((2, TOK), jnp.int32),
            pltpu.VMEM((2, TOK), F32),
            pltpu.VMEM((TOK, 160), BF),
            pltpu.VMEM((TOK, 96), BF),
            pltpu.VMEM((32, TOK), BF),
            pltpu.VMEM((TOK, 512), BF),
            pltpu.VMEM((1, 512), F32),
            pltpu.VMEM((TOK, 128), BF),
            pltpu.SemaphoreType.DMA((8,)),
        ],
    )
    arrived = swap_all(payload.reshape(N_SP, ROWS // 2, 2, 128), SP).reshape(N_SP * ROWS, 128)
    (spread,) = run(spread_kernel, [(N_TP, 272, 128)], arrived)
    latents = swap_all(spread, "tp")
    (slots,) = run(slots_kernel, [(SLOTS, 512)], arrived)
    (own,) = run(keys_kernel, [(4, N_TP * TOK, 128)], latents, wide_kv_weight, narrow_kv_weight)
    other = lax.ppermute(own, "c", [(0, 1), (1, 0)])
    state = run(attend_own_kernel, [(2, SLOTS, 128)] * 3, core, slots, own, scalars=1, kind=F32)
    (partial,) = run(
        attend_rest_kernel, [(N_TP, SLOTS, 128)],
        core, slots, other, *state, wide_out_weight, narrow_out_weight,
        scalars=1,
    )
    (copies,) = run(stream_kernel, [(N_TP, SLOTS, 128)], swap_all(partial, "tp"), slots)
    rows = swap_all(copies, "tp")
    (partial,) = run(
        expert_kernel, [(N_TP, SLOTS, 128)],
        rows, slots, norm_gain[None, :],
        expert_gate.swapaxes(1, 2), expert_up.swapaxes(1, 2), expert_down.reshape(128, D_MODEL),
        shared_gate.T, shared_up.T, shared_down,
    )
    (back,) = run(give_back_kernel, [(SLOTS, 128)], swap_all(partial, "tp"), copies, slots)
    back = swap_all(back.reshape(N_SP, 3, 2, 128), SP).reshape(SLOTS, 128)
    return run(finish_kernel, [(TOK, 128)], chosen, back, spread=False)


def solution(mesh):
    torus = Mesh(mesh.devices.reshape(16, 2, mesh.shape["tp"]), ("z", "c", "tp"))
    return jax.shard_map(
        local,
        mesh=torus,
        in_specs=(
            P(SP, "tp"),
            P(SP, "tp"),
            P(SP, None),
            P(SP, None),
            P(),
            P(None, "tp"),
            P(None, "tp"),
            P("tp", None),
            P("tp", None),
            P(SP, None),
            P(),
            P(SP, None),
            P(SP, None),
            P(SP, None, "tp"),
            P(SP, None, "tp"),
            P(SP, "tp", None),
            P(None, "tp"),
            P(None, "tp"),
            P("tp", None),
        ),
        out_specs=P(SP, "tp"),
        check_vma=False,
    )
```

```python
import functools

import jax
import jax.numpy as jnp
from jax import lax
from jax.experimental import pallas as pl
from jax.experimental.pallas import tpu as pltpu
from jax.sharding import Mesh
from jax.sharding import PartitionSpec as P

D_MODEL = 2048
THETA = 10000.0
EPS = 1e-06
FLOOR = -1e30
MESH = ("z3", "z2", "z1", "z0", "c", "y1", "y0", "x1", "x0")
SP, TP = MESH[:5], MESH[5:]
SP_ORDER = ("z0", "c", "z3", "z2", "z1")
TP_ORDER = ("y0", "x0", "y1", "x1")
N_SP = 32
N_TP = 16
TOK = 64
SLOTS = 192
F32 = jnp.float32
BF = jnp.bfloat16

ROWS = 28
LANE_POS, LANE_HI, LANE_LO, LANE_FLAG = 64, 65, 66, 67


def iota(shape, dim):
    return lax.broadcasted_iota(jnp.int32, shape, dim)


def div6(v):
    return (v * 10923) >> 16


def div3(v):
    return (v * 21846) >> 16


def div28(v):
    return (v * 2341) >> 16


def dot(a, b):
    return jnp.dot(a, b, preferred_element_type=F32)


def dot_nt(a, b):
    return lax.dot_general(a, b, (((1,), (1,)), ((), ())), preferred_element_type=F32)


def dot_tn(a, b):
    return lax.dot_general(a, b, (((0,), (0,)), ((), ())), preferred_element_type=F32)


def exact_tn(a, b):
    return lax.dot_general(
        a, b, (((0,), (0,)), ((), ())), precision=lax.Precision.HIGHEST, preferred_element_type=F32
    )


def reordered(peer, order, names):
    bits = [((peer >> (len(order) - 1 - i)) & 1) << (len(names) - 1 - names.index(axis)) for i, axis in enumerate(order)]
    return sum(bits[1:], bits[0])


def source_of(peer):
    return reordered(peer, SP_ORDER, SP)


TP_PLACES = tuple(reordered(piece, TP_ORDER, TP) for piece in range(N_TP))


def columns(piece):
    return slice(TP_PLACES[piece] * 128, (TP_PLACES[piece] + 1) * 128)


def picks(mask):
    return jnp.where(mask, 1.0, 0.0).astype(BF)


def side_value(block, lane):
    row = iota((SLOTS, 1), 0)
    return jnp.sum(jnp.where(iota(block.shape, 1) == lane + 4 * (row - 3 * div3(row)), block, 0.0), axis=1, keepdims=True)


def from_rows(source, row):
    count = source.shape[0]
    return picks(iota((count, N_SP * ROWS), 1) == source * ROWS + row)


def pack_kernel(
    tp_ref, wide_hbm, narrow_hbm, rope_hbm, lat_hbm, gain_hbm, res_hbm, ids_hbm, w_hbm, cos_ref, sin_ref, out_ref, sel_ref,
    ids_ref, w_ref, wide_ref, narrow_ref, rope_ref, lat_ref, gain_ref, res_ref, sems,
):
    t = tp_ref[0]
    own_columns = res_hbm.at[:, pl.ds(pl.multiple_of(t * 128, 128), 128)]
    sources = (ids_hbm, w_hbm, wide_hbm, narrow_hbm, rope_hbm, lat_hbm, gain_hbm, own_columns)
    targets = (ids_ref, w_ref, wide_ref, narrow_ref, rope_ref, lat_ref, gain_ref, res_ref)
    copies = [pltpu.make_async_copy(a, b, sems.at[i]) for i, (a, b) in enumerate(zip(sources, targets))]
    for copy in copies:
        copy.start()
    src, dst = iota((16, 128), 0), iota((16, 128), 1)
    turning = (dst < 32) | (dst >= 96)
    spread = jnp.where(turning & ((dst & 15) == src), 1.0, 0.0)
    cos = exact_tn(cos_ref[...], spread) + jnp.where((iota((TOK, 128), 1) >= 32) & (iota((TOK, 128), 1) < 96), 1.0, 0.0)
    sin = exact_tn(sin_ref[...], jnp.where((dst & 16) == 0, -spread, spread))
    src, dst = iota((128, 128), 0), iota((128, 128), 1)
    swap = picks(src == dst + jnp.where((dst & 16) == 0, 16, -16))
    first, after = picks(src == dst), picks(src + 32 == dst)
    twice = picks((iota((TOK, 128), 1) & 63) == iota((TOK, 128), 0))
    row = iota((4 * ROWS, 128), 0)
    peer = div28(row)
    place = row - peer * ROWS
    dest = source_of(peer)
    kind = div6(place)
    slot = dest * 6 + place - kind * 6
    lanes = iota((4 * ROWS, 128), 1)
    start = t * 2 + (place & 1)
    block = (place >> 1) - 9
    want_query = jnp.where(kind < 2, slot + kind * 1024, -100000)
    want_rest = jnp.where(kind == 2, slot, -100000)
    want_side = jnp.where(place >= 26, dest * 2 + place - 26 + 1024, -100000)
    lat_masks = [
        [picks(lanes == jnp.where((block >> 1) == pair, start + half * 32 + (block & 1) * 64, -1)) for pair in range(2)]
        for half in range(2)
    ]

    copies[0].wait()
    copies[1].wait()
    before = picks(iota((TOK, TOK), 0) < iota((TOK, TOK), 1))
    named = [jnp.where(ids_ref[k : k + 1, :] == iota((TOK, TOK), 0), 1.0, 0.0) for k in range(2)]
    rank = dot((named[0] + named[1]).astype(BF), before)
    slots = [
        ids_ref[k : k + 1, :] * 3 + jnp.sum(named[k] * rank, axis=0, keepdims=True).astype(jnp.int32) for k in range(2)
    ]

    def either(want):
        return picks((slots[0] == want) | (slots[1] == want))

    place = iota((SLOTS, TOK), 0)
    peer = div6(place)
    sel_ref[...] = either(source_of(peer) * 6 + place - peer * 6)
    lane, token = iota((TOK, 128), 1), iota((TOK, 128), 0).astype(F32)
    expert = iota((TOK, TOK), 0)
    side = 0.0
    for third in range(3):
        high, low, flag = 0.0, 0.0, 0.0
        for k in range(2):
            mask = slots[k] == expert * 3 + third
            w = w_ref[k : k + 1, :]
            w_hi = w.astype(BF).astype(F32)
            high = high + jnp.where(mask, w_hi, 0.0)
            low = low + jnp.where(mask, w - w_hi, 0.0)
            flag = flag + jnp.where(mask, 1.0 - k, 0.0)
        at = lane - 4 * third
        side = side + dot(either(expert * 3 + third), jnp.where(at == LANE_POS, token, 0.0).astype(BF))
        side = side + dot(high.astype(BF), picks(at == LANE_HI)) + dot(low.astype(BF), picks(at == LANE_LO))
        side = side + dot(flag.astype(BF), picks(at == LANE_FLAG))
    keys = [dot(slot.astype(F32).astype(BF), twice).astype(jnp.int32) for slot in slots]
    upper = iota((1, 128), 1) >= 64
    query_keys = [jnp.where(upper, key + 1024, key) for key in keys]
    rest_keys = [jnp.where(upper, -1, key) for key in keys]
    side_key = jnp.where(upper, (iota((1, 128), 1) & 63) + 1024, -1)

    for copy in copies[2:]:
        copy.wait()

    def turned(block):
        return (block.astype(F32) * cos + dot(block, swap) * sin).astype(BF)

    q_rest = turned((dot(wide_ref[:, 128:], first[:32]) + dot(narrow_ref[...], after[:96])).astype(BF))
    rope = turned(dot_tn(rope_ref[...], first[:32]).astype(BF))
    lat = lat_ref[...].astype(F32)
    scaled = lat * lax.rsqrt(jnp.mean(lat * lat, axis=1, keepdims=True) + EPS)
    normed = (scaled * gain_ref[...]).astype(BF)
    side = side + dot(picks(iota((TOK, TOK), 1) == ((expert >> 1) & 1) * 32 + t * 2 + (expert & 1)), rope)
    lat_rows = [
        jnp.concatenate([normed[:, f * 128 : (f + 1) * 128] for f in (2 * pair, 2 * pair + 1)], axis=0) for pair in range(2)
    ]
    lat_parts = [dot(masks[0], lat_rows[0]) + dot(masks[1], lat_rows[1]) for masks in lat_masks]
    query_rows = jnp.concatenate([wide_ref[:, :128], q_rest], axis=0)
    rest_rows = jnp.concatenate([res_ref[...], side.astype(BF)], axis=0)
    for part in range(N_SP // 4):
        away = source_of(4 * part)
        want = want_query + 6 * away
        out = dot(picks((query_keys[0] == want) | (query_keys[1] == want)), query_rows)
        want = want_rest + 6 * away
        mask = (rest_keys[0] == want) | (rest_keys[1] == want) | (side_key == want_side + 2 * away)
        out = out + dot(picks(mask), rest_rows)
        out_ref[part * 4 * ROWS : (part + 1) * 4 * ROWS, :] = (out + lat_parts[away & 1]).astype(BF)


def slots_kernel(arr_ref, out_ref):
    row = iota((SLOTS, 1), 0)
    source = div6(row)
    place = row - source * 6
    for i, start in enumerate((place, place + 6, place + 12, 26 + div3(place))):
        out_ref[:, i * 128 : (i + 1) * 128] = dot(from_rows(source, start), arr_ref[...]).astype(BF)


def spread_kernel(arr_ref, out_ref):
    n = iota((TOK, 1), 0)
    rows = [dot(from_rows(n >> 1, 18 + 2 * f + (n & 1)), arr_ref[...]).astype(BF) for f in range(4)]
    rope = dot(from_rows(n >> 1, 26 + (n & 1)), arr_ref[...]).astype(BF)
    packed = jnp.zeros((16, 128), F32)
    src, dst = iota((128, 128), 0), iota((128, 128), 1)
    for b in range(4):
        packed = packed + dot(rope[16 * b : 16 * (b + 1)], picks((src < 32) & (dst == src + 32 * b)))
    packed = packed.astype(BF)
    for copy in range(N_TP):
        for f in range(4):
            out_ref[copy, f * TOK : (f + 1) * TOK, :] = rows[f]
        out_ref[copy, 4 * TOK :, :] = packed


def keys_kernel(lat_ref, wide_ref, narrow_ref, out_ref):
    rows = N_TP * TOK
    wide = jnp.zeros((rows, 256), F32)
    narrow = jnp.zeros((rows, 128), F32)
    for pair in range(2):
        parts = [lat_ref[:, f * TOK : (f + 1) * TOK, :].reshape(rows, 128) for f in (2 * pair, 2 * pair + 1)]
        part = jnp.concatenate(parts, axis=1)
        wide = wide + dot(part, wide_ref[pair * 256 : (pair + 1) * 256, :])
        narrow = narrow + dot(part, narrow_ref[pair * 256 : (pair + 1) * 256, :])
    wide, narrow = wide.astype(BF), narrow.astype(BF)
    packed = lat_ref[:, 4 * TOK :, :].reshape(256, 128)
    src, dst = iota((128, 128), 0), iota((128, 128), 1)
    pieces = []
    for b in range(4):
        moved = dot(packed, picks((dst >= 96) & (src == dst - 96 + 32 * b)))
        pieces.append(moved.astype(BF).reshape(N_TP, 16, 128))
    rope = jnp.concatenate(pieces, axis=1).reshape(rows, 128)
    out_ref[0] = wide[:, :128]
    out_ref[1] = wide[:, 128:]
    shifted = dot(narrow, picks((src < 64) & (dst == src + 32)))
    out_ref[2] = (shifted + rope.astype(F32)).astype(BF)
    out_ref[3] = dot(narrow, picks((src >= 64) & (dst == src - 64))).astype(BF)


def half_attention(half, slot_ref, kv_ref):
    q = slot_ref[:, :256]
    side = slot_ref[:, 384:].astype(F32)
    row_pos = source_of(div6(iota((SLOTS, 1), 0))) * TOK + side_value(side, LANE_POS).astype(jnp.int32)
    src, dst = iota((128, 128), 0), iota((128, 128), 1)
    q_rest = q[:, 128:]
    wide_q = jnp.concatenate([q[:, :128], dot(q_rest, picks((src < 32) & (dst == src + 96))).astype(BF)], axis=1)
    narrow_q = jnp.where(iota((SLOTS, 128), 1) >= 32, q_rest.astype(F32), 0.0).astype(BF)
    n = iota((1, N_TP * TOK), 1)
    source, taken = source_of((n & 63) >> 1), reordered(n >> 6, TP_ORDER, TP)
    allowed = source * TOK + taken * 2 + (n & 1) + half * 32 <= row_pos
    wide = dot_nt(wide_q, jnp.concatenate([kv_ref[0], kv_ref[2]], axis=1)) * (160 ** -0.5)
    narrow = dot_nt(narrow_q, kv_ref[2]) * (96 ** -0.5)
    return [jnp.where(allowed, s, FLOOR) for s in (wide, narrow)]


def weighed(scores, peak, values):
    e = jnp.exp(scores - peak)
    return jnp.sum(e, axis=1, keepdims=True), dot(e.astype(BF), values)


def attend_own_kernel(core_ref, slot_ref, kv_ref, peak_ref, total_ref, sum_ref):
    for i, scores in enumerate(half_attention(core_ref[0], slot_ref, kv_ref)):
        peak = jnp.max(scores, axis=1, keepdims=True)
        total, summed = weighed(scores, peak, kv_ref[1 + 2 * i])
        peak_ref[i] = jnp.broadcast_to(peak, (SLOTS, 128))
        total_ref[i] = jnp.broadcast_to(total, (SLOTS, 128))
        sum_ref[i] = summed


def attend_rest_kernel(core_ref, slot_ref, kv_ref, peak_ref, total_ref, sum_ref, wide_out_ref, narrow_out_ref, out_ref):
    attended = []
    for i, scores in enumerate(half_attention(1 - core_ref[0], slot_ref, kv_ref)):
        old = peak_ref[i][:, :1]
        peak = jnp.maximum(old, jnp.max(scores, axis=1, keepdims=True))
        total, summed = weighed(scores, peak, kv_ref[1 + 2 * i])
        kept = jnp.exp(old - peak)
        attended.append(((summed + kept * sum_ref[i]) / (total + kept * total_ref[i][:, :1])).astype(BF))
    wide_att, narrow_att = attended[0], attended[1][:, :64]
    for pair in range(N_TP // 2):
        ends = columns(2 * pair), columns(2 * pair + 1)
        wide, narrow = (jnp.concatenate([ref[:, c] for c in ends], axis=1) for ref in (wide_out_ref, narrow_out_ref))
        both = (dot(wide_att, wide) + dot(narrow_att, narrow)).astype(BF)
        out_ref[2 * pair] = both[:, :128]
        out_ref[2 * pair + 1] = both[:, 128:]


def stream_kernel(part_ref, slot_ref, out_ref):
    total = jnp.zeros((SLOTS, 128), F32)
    for piece in range(N_TP):
        total = total + part_ref[piece].astype(F32)
    stream = (slot_ref[:, 256:384].astype(F32) + total.astype(BF).astype(F32)).astype(BF)
    for copy in range(N_TP):
        out_ref[copy] = stream


def expert_kernel(x_ref, slot_ref, gain_ref, eg_ref, eu_ref, ed_ref, sg_ref, su_ref, sd_ref, out_ref):
    squares = jnp.zeros((SLOTS, 128), F32)
    for piece in range(N_TP):
        x = x_ref[piece].astype(F32)
        squares = squares + x * x
    scale = lax.rsqrt(jnp.sum(squares, axis=1, keepdims=True) * (1.0 / D_MODEL) + EPS)
    into = jnp.zeros((SLOTS, 384), F32)
    for pair in range(N_TP // 2):
        ends = columns(2 * pair), columns(2 * pair + 1)
        x = jnp.concatenate([x_ref[2 * pair], x_ref[2 * pair + 1]], axis=1).astype(F32)
        x = (x * scale * jnp.concatenate([gain_ref[:, c] for c in ends], axis=1)).astype(BF)
        halves = [
            jnp.concatenate([eg_ref[0, :, c], eg_ref[1, :, c], sg_ref[:, c], eu_ref[0, :, c], eu_ref[1, :, c], su_ref[:, c]], axis=0)
            for c in ends
        ]
        into = into + dot_nt(x, jnp.concatenate(halves, axis=1))
    gate, up = into[:, :192], into[:, 192:]
    hidden = (gate / (1.0 + jnp.exp(-gate))) * up
    side = slot_ref[:, 384:].astype(F32)
    weight = side_value(side, LANE_HI) + side_value(side, LANE_LO)
    flag = side_value(side, LANE_FLAG)
    owner = div3(iota((SLOTS, 128), 0)) & 1
    routed_hidden = jnp.where(owner == (iota((SLOTS, 128), 1) >> 6), hidden[:, :128], 0.0).astype(BF)
    shared_hidden = hidden[:, 128:].astype(BF)
    for pair in range(N_TP // 2):
        ends = columns(2 * pair), columns(2 * pair + 1)
        routed_down, shared_down = (jnp.concatenate([ref[:, c] for c in ends], axis=1) for ref in (ed_ref, sd_ref))
        both = (weight * dot(routed_hidden, routed_down) + flag * dot(shared_hidden, shared_down)).astype(BF)
        out_ref[2 * pair] = both[:, :128]
        out_ref[2 * pair + 1] = both[:, 128:]


def give_back_kernel(part_ref, stream_ref, slot_ref, out_ref):
    total = jnp.zeros((SLOTS, 128), F32)
    for piece in range(N_TP):
        total = total + part_ref[piece].astype(F32)
    flag = side_value(slot_ref[:, 384:].astype(F32), LANE_FLAG)
    out_ref[...] = (total + flag * stream_ref[0].astype(F32)).astype(BF)


def finish_kernel(sel_ref, back_ref, out_ref):
    out_ref[...] = dot_tn(sel_ref[...], back_ref[...]).astype(BF)


VMEM = pl.BlockSpec(memory_space=pltpu.VMEM)
SMEM = pl.BlockSpec(memory_space=pltpu.SMEM)


HBM = pl.BlockSpec(memory_space=pltpu.HBM)


def run(kernel, outs, *args, scalars=0, plain=0, spread=True, kind=BF, scratch=()):
    spaces = [pltpu.HBM if i < plain else pltpu.VMEM for i in range(scalars, len(args))]
    placed = [pltpu.with_memory_space_constraint(a, m) for a, m in zip(args[scalars:], spaces)]
    args = [*args[:scalars], *placed]
    return pl.pallas_call(
        kernel,
        out_shape=[pltpu.VMEM(shape, kind) for shape in outs] if spread else jax.ShapeDtypeStruct(outs[0], BF),
        in_specs=[SMEM] * scalars + [HBM if m is pltpu.HBM else VMEM for m in spaces],
        out_specs=[VMEM] * len(outs) if spread else VMEM,
        scratch_shapes=scratch,
        compiler_params=pltpu.CompilerParams(vmem_limit_bytes=24 << 20),
        name=kernel.__name__,
    )(*args)


def swap_all(values, axes):
    return lax.all_to_all(values, axes, split_axis=0, concat_axis=0, tiled=True)


def local(
    wide_queries,
    narrow_queries,
    kv_latent,
    rope_key,
    latent_gain,
    wide_kv_weight,
    narrow_kv_weight,
    wide_out_weight,
    narrow_out_weight,
    residual,
    norm_gain,
    route_ids,
    route_weights,
    expert_gate,
    expert_up,
    expert_down,
    shared_gate,
    shared_up,
    shared_down,
):
    t = lax.axis_index(TP).astype(jnp.int32)[None]
    core = lax.axis_index("c").astype(jnp.int32)[None]
    frequency = THETA ** (-2.0 * jnp.arange(16, dtype=F32) / 32)
    positions = lax.axis_index(SP) * TOK + jnp.arange(TOK, dtype=jnp.int32)
    angles = frequency[:, None] * positions.astype(F32)[None, :]
    payload, chosen = run(
        pack_kernel, [(N_SP * ROWS, 128), (SLOTS, TOK)],
        t, wide_queries, narrow_queries, rope_key.T, kv_latent, latent_gain[None, :], residual,
        route_ids.T, route_weights.T, jnp.cos(angles), jnp.sin(angles),
        scalars=1,
        plain=9,
        scratch=[
            pltpu.VMEM((2, TOK), jnp.int32),
            pltpu.VMEM((2, TOK), F32),
            pltpu.VMEM((TOK, 160), BF),
            pltpu.VMEM((TOK, 96), BF),
            pltpu.VMEM((32, TOK), BF),
            pltpu.VMEM((TOK, 512), BF),
            pltpu.VMEM((1, 512), F32),
            pltpu.VMEM((TOK, 128), BF),
            pltpu.SemaphoreType.DMA((8,)),
        ],
    )
    arrived = swap_all(payload.reshape(N_SP, ROWS // 2, 2, 128), SP_ORDER).reshape(N_SP * ROWS, 128)
    (spread,) = run(spread_kernel, [(N_TP, 272, 128)], arrived)
    latents = swap_all(spread, TP_ORDER)
    (slots,) = run(slots_kernel, [(SLOTS, 512)], arrived)
    (own,) = run(keys_kernel, [(4, N_TP * TOK, 128)], latents, wide_kv_weight, narrow_kv_weight)
    other = lax.ppermute(own, "c", [(0, 1), (1, 0)])
    state = run(attend_own_kernel, [(2, SLOTS, 128)] * 3, core, slots, own, scalars=1, kind=F32)
    (partial,) = run(
        attend_rest_kernel, [(N_TP, SLOTS, 128)],
        core, slots, other, *state, wide_out_weight, narrow_out_weight,
        scalars=1,
    )
    (copies,) = run(stream_kernel, [(N_TP, SLOTS, 128)], swap_all(partial, TP_ORDER), slots)
    rows = swap_all(copies, TP_ORDER)
    (partial,) = run(
        expert_kernel, [(N_TP, SLOTS, 128)],
        rows, slots, norm_gain[None, :],
        expert_gate.swapaxes(1, 2), expert_up.swapaxes(1, 2), expert_down.reshape(128, D_MODEL),
        shared_gate.T, shared_up.T, shared_down,
    )
    (back,) = run(give_back_kernel, [(SLOTS, 128)], swap_all(partial, TP_ORDER), copies, slots)
    back = swap_all(back.reshape(N_SP, 3, 2, 128), SP_ORDER).reshape(SLOTS, 128)
    return run(finish_kernel, [(TOK, 128)], chosen, back, spread=False)


def solution(mesh):
    torus = Mesh(mesh.devices.reshape((2,) * len(MESH)), MESH)
    return jax.shard_map(
        local,
        mesh=torus,
        in_specs=(
            P(SP, TP),
            P(SP, TP),
            P(SP, None),
            P(SP, None),
            P(),
            P(None, TP),
            P(None, TP),
            P(TP, None),
            P(TP, None),
            P(SP, None),
            P(),
            P(SP, None),
            P(SP, None),
            P(SP, None, TP),
            P(SP, None, TP),
            P(SP, TP, None),
            P(None, TP),
            P(None, TP),
            P(TP, None),
        ),
        out_specs=P(SP, TP),
        check_vma=False,
    )
```

```python
import functools

import jax
import jax.numpy as jnp
from jax import lax
from jax.experimental import pallas as pl
from jax.experimental.pallas import tpu as pltpu
from jax.sharding import Mesh
from jax.sharding import PartitionSpec as P

D_MODEL = 2048
THETA = 10000.0
EPS = 1e-06
FLOOR = -1e30
MESH = ("z3", "z2", "z1", "z0", "c", "y1", "y0", "x1", "x0")
SP, TP = MESH[:5], MESH[5:]
SP_ORDER = ("c", "z1", "z0", "z3", "z2")
TP_ORDER = ("y0", "x0", "y1", "x1")
N_SP = 32
N_TP = 16
TOK = 64
SLOTS = 192
F32 = jnp.float32
BF = jnp.bfloat16

ROWS = 28
LANE_POS, LANE_HI, LANE_LO, LANE_FLAG = 64, 65, 66, 67


def iota(shape, dim):
    return lax.broadcasted_iota(jnp.int32, shape, dim)


def div6(v):
    return (v * 10923) >> 16


def div3(v):
    return (v * 21846) >> 16


def div28(v):
    return (v * 2341) >> 16


def dot(a, b):
    return jnp.dot(a, b, preferred_element_type=F32)


def dot_nt(a, b):
    return lax.dot_general(a, b, (((1,), (1,)), ((), ())), preferred_element_type=F32)


def dot_tn(a, b):
    return lax.dot_general(a, b, (((0,), (0,)), ((), ())), preferred_element_type=F32)


def exact_tn(a, b):
    return lax.dot_general(
        a, b, (((0,), (0,)), ((), ())), precision=lax.Precision.HIGHEST, preferred_element_type=F32
    )


def reordered(peer, order, names):
    bits = [((peer >> (len(order) - 1 - i)) & 1) << (len(names) - 1 - names.index(axis)) for i, axis in enumerate(order)]
    return sum(bits[1:], bits[0])


def source_of(peer):
    return reordered(peer, SP_ORDER, SP)


TP_PLACES = tuple(reordered(piece, TP_ORDER, TP) for piece in range(N_TP))


def columns(piece):
    return slice(TP_PLACES[piece] * 128, (TP_PLACES[piece] + 1) * 128)


def picks(mask):
    return jnp.where(mask, 1.0, 0.0).astype(BF)


def side_value(block, lane):
    row = iota((SLOTS, 1), 0)
    return jnp.sum(jnp.where(iota(block.shape, 1) == lane + 4 * (row - 3 * div3(row)), block, 0.0), axis=1, keepdims=True)


def from_rows(source, row):
    count = source.shape[0]
    return picks(iota((count, N_SP * ROWS), 1) == source * ROWS + row)


def pack_kernel(
    tp_ref, wide_hbm, narrow_hbm, rope_hbm, lat_hbm, gain_hbm, res_hbm, ids_hbm, w_hbm, cos_ref, sin_ref, out_ref, sel_ref,
    ids_ref, w_ref, wide_ref, narrow_ref, rope_ref, lat_ref, gain_ref, res_ref, sems,
):
    t = tp_ref[0]
    own_columns = res_hbm.at[:, pl.ds(pl.multiple_of(t * 128, 128), 128)]
    sources = (ids_hbm, w_hbm, wide_hbm, narrow_hbm, rope_hbm, lat_hbm, gain_hbm, own_columns)
    targets = (ids_ref, w_ref, wide_ref, narrow_ref, rope_ref, lat_ref, gain_ref, res_ref)
    copies = [pltpu.make_async_copy(a, b, sems.at[i]) for i, (a, b) in enumerate(zip(sources, targets))]
    for copy in copies:
        copy.start()
    src, dst = iota((16, 128), 0), iota((16, 128), 1)
    turning = (dst < 32) | (dst >= 96)
    spread = jnp.where(turning & ((dst & 15) == src), 1.0, 0.0)
    cos = exact_tn(cos_ref[...], spread) + jnp.where((iota((TOK, 128), 1) >= 32) & (iota((TOK, 128), 1) < 96), 1.0, 0.0)
    sin = exact_tn(sin_ref[...], jnp.where((dst & 16) == 0, -spread, spread))
    src, dst = iota((128, 128), 0), iota((128, 128), 1)
    swap = picks(src == dst + jnp.where((dst & 16) == 0, 16, -16))
    first, after = picks(src == dst), picks(src + 32 == dst)
    twice = picks((iota((TOK, 128), 1) & 63) == iota((TOK, 128), 0))
    row = iota((4 * ROWS, 128), 0)
    peer = div28(row)
    place = row - peer * ROWS
    dest = source_of(peer)
    kind = div6(place)
    slot = dest * 6 + place - kind * 6
    lanes = iota((4 * ROWS, 128), 1)
    start = t * 2 + (place & 1)
    block = (place >> 1) - 9
    want_query = jnp.where(kind < 2, slot + kind * 1024, -100000)
    want_rest = jnp.where(kind == 2, slot, -100000)
    want_side = jnp.where(place >= 26, dest * 2 + place - 26 + 1024, -100000)
    lat_masks = [
        [picks(lanes == jnp.where((block >> 1) == pair, start + half * 32 + (block & 1) * 64, -1)) for pair in range(2)]
        for half in range(2)
    ]

    copies[0].wait()
    copies[1].wait()
    before = picks(iota((TOK, TOK), 0) < iota((TOK, TOK), 1))
    named = [jnp.where(ids_ref[k : k + 1, :] == iota((TOK, TOK), 0), 1.0, 0.0) for k in range(2)]
    rank = dot((named[0] + named[1]).astype(BF), before)
    slots = [
        ids_ref[k : k + 1, :] * 3 + jnp.sum(named[k] * rank, axis=0, keepdims=True).astype(jnp.int32) for k in range(2)
    ]

    def either(want):
        return picks((slots[0] == want) | (slots[1] == want))

    place = iota((SLOTS, TOK), 0)
    peer = div6(place)
    sel_ref[...] = either(source_of(peer) * 6 + place - peer * 6)
    lane, token = iota((TOK, 128), 1), iota((TOK, 128), 0).astype(F32)
    expert = iota((TOK, TOK), 0)
    side = 0.0
    for third in range(3):
        high, low, flag = 0.0, 0.0, 0.0
        for k in range(2):
            mask = slots[k] == expert * 3 + third
            w = w_ref[k : k + 1, :]
            w_hi = w.astype(BF).astype(F32)
            high = high + jnp.where(mask, w_hi, 0.0)
            low = low + jnp.where(mask, w - w_hi, 0.0)
            flag = flag + jnp.where(mask, 1.0 - k, 0.0)
        at = lane - 4 * third
        side = side + dot(either(expert * 3 + third), jnp.where(at == LANE_POS, token, 0.0).astype(BF))
        side = side + dot(high.astype(BF), picks(at == LANE_HI)) + dot(low.astype(BF), picks(at == LANE_LO))
        side = side + dot(flag.astype(BF), picks(at == LANE_FLAG))
    keys = [dot(slot.astype(F32).astype(BF), twice).astype(jnp.int32) for slot in slots]
    upper = iota((1, 128), 1) >= 64
    query_keys = [jnp.where(upper, key + 1024, key) for key in keys]
    rest_keys = [jnp.where(upper, -1, key) for key in keys]
    side_key = jnp.where(upper, (iota((1, 128), 1) & 63) + 1024, -1)

    for copy in copies[2:]:
        copy.wait()

    def turned(block):
        return (block.astype(F32) * cos + dot(block, swap) * sin).astype(BF)

    q_rest = turned((dot(wide_ref[:, 128:], first[:32]) + dot(narrow_ref[...], after[:96])).astype(BF))
    rope = turned(dot_tn(rope_ref[...], first[:32]).astype(BF))
    lat = lat_ref[...].astype(F32)
    scaled = lat * lax.rsqrt(jnp.mean(lat * lat, axis=1, keepdims=True) + EPS)
    normed = (scaled * gain_ref[...]).astype(BF)
    side = side + dot(picks(iota((TOK, TOK), 1) == ((expert >> 1) & 1) * 32 + t * 2 + (expert & 1)), rope)
    lat_rows = [
        jnp.concatenate([normed[:, f * 128 : (f + 1) * 128] for f in (2 * pair, 2 * pair + 1)], axis=0) for pair in range(2)
    ]
    lat_parts = [dot(masks[0], lat_rows[0]) + dot(masks[1], lat_rows[1]) for masks in lat_masks]
    query_rows = jnp.concatenate([wide_ref[:, :128], q_rest], axis=0)
    rest_rows = jnp.concatenate([res_ref[...], side.astype(BF)], axis=0)
    for part in range(N_SP // 4):
        away = source_of(4 * part)
        want = want_query + 6 * away
        out = dot(picks((query_keys[0] == want) | (query_keys[1] == want)), query_rows)
        want = want_rest + 6 * away
        mask = (rest_keys[0] == want) | (rest_keys[1] == want) | (side_key == want_side + 2 * away)
        out = out + dot(picks(mask), rest_rows)
        out_ref[part * 4 * ROWS : (part + 1) * 4 * ROWS, :] = (out + lat_parts[away & 1]).astype(BF)


def slots_kernel(arr_ref, out_ref):
    row = iota((SLOTS, 1), 0)
    source = div6(row)
    place = row - source * 6
    for i, start in enumerate((place, place + 6, place + 12, 26 + div3(place))):
        out_ref[:, i * 128 : (i + 1) * 128] = dot(from_rows(source, start), arr_ref[...]).astype(BF)


def spread_kernel(arr_ref, out_ref):
    n = iota((TOK, 1), 0)
    rows = [dot(from_rows(n >> 1, 18 + 2 * f + (n & 1)), arr_ref[...]).astype(BF) for f in range(4)]
    rope = dot(from_rows(n >> 1, 26 + (n & 1)), arr_ref[...]).astype(BF)
    packed = jnp.zeros((16, 128), F32)
    src, dst = iota((128, 128), 0), iota((128, 128), 1)
    for b in range(4):
        packed = packed + dot(rope[16 * b : 16 * (b + 1)], picks((src < 32) & (dst == src + 32 * b)))
    packed = packed.astype(BF)
    for copy in range(N_TP):
        for f in range(4):
            out_ref[copy, f * TOK : (f + 1) * TOK, :] = rows[f]
        out_ref[copy, 4 * TOK :, :] = packed


def keys_kernel(lat_ref, wide_ref, narrow_ref, out_ref):
    rows = N_TP * TOK
    wide = jnp.zeros((rows, 256), F32)
    narrow = jnp.zeros((rows, 128), F32)
    for pair in range(2):
        parts = [lat_ref[:, f * TOK : (f + 1) * TOK, :].reshape(rows, 128) for f in (2 * pair, 2 * pair + 1)]
        part = jnp.concatenate(parts, axis=1)
        wide = wide + dot(part, wide_ref[pair * 256 : (pair + 1) * 256, :])
        narrow = narrow + dot(part, narrow_ref[pair * 256 : (pair + 1) * 256, :])
    wide, narrow = wide.astype(BF), narrow.astype(BF)
    packed = lat_ref[:, 4 * TOK :, :].reshape(256, 128)
    src, dst = iota((128, 128), 0), iota((128, 128), 1)
    pieces = []
    for b in range(4):
        moved = dot(packed, picks((dst >= 96) & (src == dst - 96 + 32 * b)))
        pieces.append(moved.astype(BF).reshape(N_TP, 16, 128))
    rope = jnp.concatenate(pieces, axis=1).reshape(rows, 128)
    out_ref[0] = wide[:, :128]
    out_ref[1] = wide[:, 128:]
    shifted = dot(narrow, picks((src < 64) & (dst == src + 32)))
    out_ref[2] = (shifted + rope.astype(F32)).astype(BF)
    out_ref[3] = dot(narrow, picks((src >= 64) & (dst == src - 64))).astype(BF)


def half_attention(half, slot_ref, kv_ref):
    q = slot_ref[:, :256]
    side = slot_ref[:, 384:].astype(F32)
    row_pos = source_of(div6(iota((SLOTS, 1), 0))) * TOK + side_value(side, LANE_POS).astype(jnp.int32)
    src, dst = iota((128, 128), 0), iota((128, 128), 1)
    q_rest = q[:, 128:]
    wide_q = jnp.concatenate([q[:, :128], dot(q_rest, picks((src < 32) & (dst == src + 96))).astype(BF)], axis=1)
    narrow_q = jnp.where(iota((SLOTS, 128), 1) >= 32, q_rest.astype(F32), 0.0).astype(BF)
    n = iota((1, N_TP * TOK), 1)
    source, taken = source_of((n & 63) >> 1), reordered(n >> 6, TP_ORDER, TP)
    allowed = source * TOK + taken * 2 + (n & 1) + half * 32 <= row_pos
    wide = dot_nt(wide_q, jnp.concatenate([kv_ref[0], kv_ref[2]], axis=1)) * (160 ** -0.5)
    narrow = dot_nt(narrow_q, kv_ref[2]) * (96 ** -0.5)
    return [jnp.where(allowed, s, FLOOR) for s in (wide, narrow)]


def weighed(scores, peak, values):
    e = jnp.exp(scores - peak)
    return jnp.sum(e, axis=1, keepdims=True), dot(e.astype(BF), values)


def attend_own_kernel(core_ref, slot_ref, kv_ref, peak_ref, total_ref, sum_ref):
    for i, scores in enumerate(half_attention(core_ref[0], slot_ref, kv_ref)):
        peak = jnp.max(scores, axis=1, keepdims=True)
        total, summed = weighed(scores, peak, kv_ref[1 + 2 * i])
        peak_ref[i] = jnp.broadcast_to(peak, (SLOTS, 128))
        total_ref[i] = jnp.broadcast_to(total, (SLOTS, 128))
        sum_ref[i] = summed


def attend_rest_kernel(core_ref, slot_ref, kv_ref, peak_ref, total_ref, sum_ref, wide_out_ref, narrow_out_ref, out_ref):
    attended = []
    for i, scores in enumerate(half_attention(1 - core_ref[0], slot_ref, kv_ref)):
        old = peak_ref[i][:, :1]
        peak = jnp.maximum(old, jnp.max(scores, axis=1, keepdims=True))
        total, summed = weighed(scores, peak, kv_ref[1 + 2 * i])
        kept = jnp.exp(old - peak)
        attended.append(((summed + kept * sum_ref[i]) / (total + kept * total_ref[i][:, :1])).astype(BF))
    wide_att, narrow_att = attended[0], attended[1][:, :64]
    for pair in range(N_TP // 2):
        ends = columns(2 * pair), columns(2 * pair + 1)
        wide, narrow = (jnp.concatenate([ref[:, c] for c in ends], axis=1) for ref in (wide_out_ref, narrow_out_ref))
        both = (dot(wide_att, wide) + dot(narrow_att, narrow)).astype(BF)
        out_ref[2 * pair] = both[:, :128]
        out_ref[2 * pair + 1] = both[:, 128:]


def stream_kernel(part_ref, slot_ref, out_ref):
    total = jnp.zeros((SLOTS, 128), F32)
    for piece in range(N_TP):
        total = total + part_ref[piece].astype(F32)
    stream = (slot_ref[:, 256:384].astype(F32) + total.astype(BF).astype(F32)).astype(BF)
    for copy in range(N_TP):
        out_ref[copy] = stream


def expert_kernel(x_ref, slot_ref, gain_ref, eg_ref, eu_ref, ed_ref, sg_ref, su_ref, sd_ref, out_ref):
    squares = jnp.zeros((SLOTS, 128), F32)
    for piece in range(N_TP):
        x = x_ref[piece].astype(F32)
        squares = squares + x * x
    scale = lax.rsqrt(jnp.sum(squares, axis=1, keepdims=True) * (1.0 / D_MODEL) + EPS)
    into = jnp.zeros((SLOTS, 384), F32)
    for pair in range(N_TP // 2):
        ends = columns(2 * pair), columns(2 * pair + 1)
        x = jnp.concatenate([x_ref[2 * pair], x_ref[2 * pair + 1]], axis=1).astype(F32)
        x = (x * scale * jnp.concatenate([gain_ref[:, c] for c in ends], axis=1)).astype(BF)
        halves = [
            jnp.concatenate([eg_ref[0, :, c], eg_ref[1, :, c], sg_ref[:, c], eu_ref[0, :, c], eu_ref[1, :, c], su_ref[:, c]], axis=0)
            for c in ends
        ]
        into = into + dot_nt(x, jnp.concatenate(halves, axis=1))
    gate, up = into[:, :192], into[:, 192:]
    hidden = (gate / (1.0 + jnp.exp(-gate))) * up
    side = slot_ref[:, 384:].astype(F32)
    weight = side_value(side, LANE_HI) + side_value(side, LANE_LO)
    flag = side_value(side, LANE_FLAG)
    owner = div3(iota((SLOTS, 128), 0)) & 1
    routed_hidden = jnp.where(owner == (iota((SLOTS, 128), 1) >> 6), hidden[:, :128], 0.0).astype(BF)
    shared_hidden = hidden[:, 128:].astype(BF)
    for pair in range(N_TP // 2):
        ends = columns(2 * pair), columns(2 * pair + 1)
        routed_down, shared_down = (jnp.concatenate([ref[:, c] for c in ends], axis=1) for ref in (ed_ref, sd_ref))
        both = (weight * dot(routed_hidden, routed_down) + flag * dot(shared_hidden, shared_down)).astype(BF)
        out_ref[2 * pair] = both[:, :128]
        out_ref[2 * pair + 1] = both[:, 128:]


def give_back_kernel(part_ref, stream_ref, slot_ref, out_ref):
    total = jnp.zeros((SLOTS, 128), F32)
    for piece in range(N_TP):
        total = total + part_ref[piece].astype(F32)
    flag = side_value(slot_ref[:, 384:].astype(F32), LANE_FLAG)
    out_ref[...] = (total + flag * stream_ref[0].astype(F32)).astype(BF)


def finish_kernel(sel_ref, back_ref, out_ref):
    out_ref[...] = dot_tn(sel_ref[...], back_ref[...]).astype(BF)


VMEM = pl.BlockSpec(memory_space=pltpu.VMEM)
SMEM = pl.BlockSpec(memory_space=pltpu.SMEM)


HBM = pl.BlockSpec(memory_space=pltpu.HBM)


def run(kernel, outs, *args, scalars=0, plain=0, spread=True, kind=BF, scratch=()):
    spaces = [pltpu.HBM if i < plain else pltpu.VMEM for i in range(scalars, len(args))]
    placed = [pltpu.with_memory_space_constraint(a, m) for a, m in zip(args[scalars:], spaces)]
    args = [*args[:scalars], *placed]
    return pl.pallas_call(
        kernel,
        out_shape=[pltpu.VMEM(shape, kind) for shape in outs] if spread else jax.ShapeDtypeStruct(outs[0], BF),
        in_specs=[SMEM] * scalars + [HBM if m is pltpu.HBM else VMEM for m in spaces],
        out_specs=[VMEM] * len(outs) if spread else VMEM,
        scratch_shapes=scratch,
        compiler_params=pltpu.CompilerParams(vmem_limit_bytes=24 << 20),
        name=kernel.__name__,
    )(*args)


def swap_all(values, axes):
    return lax.all_to_all(values, axes, split_axis=0, concat_axis=0, tiled=True)


def local(
    wide_queries,
    narrow_queries,
    kv_latent,
    rope_key,
    latent_gain,
    wide_kv_weight,
    narrow_kv_weight,
    wide_out_weight,
    narrow_out_weight,
    residual,
    norm_gain,
    route_ids,
    route_weights,
    expert_gate,
    expert_up,
    expert_down,
    shared_gate,
    shared_up,
    shared_down,
):
    t = lax.axis_index(TP).astype(jnp.int32)[None]
    core = lax.axis_index("c").astype(jnp.int32)[None]
    frequency = THETA ** (-2.0 * jnp.arange(16, dtype=F32) / 32)
    positions = lax.axis_index(SP) * TOK + jnp.arange(TOK, dtype=jnp.int32)
    angles = frequency[:, None] * positions.astype(F32)[None, :]
    payload, chosen = run(
        pack_kernel, [(N_SP * ROWS, 128), (SLOTS, TOK)],
        t, wide_queries, narrow_queries, rope_key.T, kv_latent, latent_gain[None, :], residual,
        route_ids.T, route_weights.T, jnp.cos(angles), jnp.sin(angles),
        scalars=1,
        plain=9,
        scratch=[
            pltpu.VMEM((2, TOK), jnp.int32),
            pltpu.VMEM((2, TOK), F32),
            pltpu.VMEM((TOK, 160), BF),
            pltpu.VMEM((TOK, 96), BF),
            pltpu.VMEM((32, TOK), BF),
            pltpu.VMEM((TOK, 512), BF),
            pltpu.VMEM((1, 512), F32),
            pltpu.VMEM((TOK, 128), BF),
            pltpu.SemaphoreType.DMA((8,)),
        ],
    )
    arrived = swap_all(payload.reshape(N_SP, ROWS // 2, 2, 128), SP_ORDER).reshape(N_SP * ROWS, 128)
    (spread,) = run(spread_kernel, [(N_TP, 272, 128)], arrived)
    latents = swap_all(spread, TP_ORDER)
    (slots,) = run(slots_kernel, [(SLOTS, 512)], arrived)
    (own,) = run(keys_kernel, [(4, N_TP * TOK, 128)], latents, wide_kv_weight, narrow_kv_weight)
    other = lax.ppermute(own, "c", [(0, 1), (1, 0)])
    state = run(attend_own_kernel, [(2, SLOTS, 128)] * 3, core, slots, own, scalars=1, kind=F32)
    (partial,) = run(
        attend_rest_kernel, [(N_TP, SLOTS, 128)],
        core, slots, other, *state, wide_out_weight, narrow_out_weight,
        scalars=1,
    )
    (copies,) = run(stream_kernel, [(N_TP, SLOTS, 128)], swap_all(partial, TP_ORDER), slots)
    rows = swap_all(copies, TP_ORDER)
    (partial,) = run(
        expert_kernel, [(N_TP, SLOTS, 128)],
        rows, slots, norm_gain[None, :],
        expert_gate.swapaxes(1, 2), expert_up.swapaxes(1, 2), expert_down.reshape(128, D_MODEL),
        shared_gate.T, shared_up.T, shared_down,
    )
    (back,) = run(give_back_kernel, [(SLOTS, 128)], swap_all(partial, TP_ORDER), copies, slots)
    back = swap_all(back.reshape(N_SP, 3, 2, 128), SP_ORDER).reshape(SLOTS, 128)
    return run(finish_kernel, [(TOK, 128)], chosen, back, spread=False)


def solution(mesh):
    torus = Mesh(mesh.devices.reshape((2,) * len(MESH)), MESH)
    return jax.shard_map(
        local,
        mesh=torus,
        in_specs=(
            P(SP, TP),
            P(SP, TP),
            P(SP, None),
            P(SP, None),
            P(),
            P(None, TP),
            P(None, TP),
            P(TP, None),
            P(TP, None),
            P(SP, None),
            P(),
            P(SP, None),
            P(SP, None),
            P(SP, None, TP),
            P(SP, None, TP),
            P(SP, TP, None),
            P(None, TP),
            P(None, TP),
            P(TP, None),
        ),
        out_specs=P(SP, TP),
        check_vma=False,
    )
```

```python
import functools

import jax
import jax.numpy as jnp
from jax import lax
from jax.experimental import pallas as pl
from jax.experimental.pallas import tpu as pltpu
from jax.sharding import Mesh
from jax.sharding import PartitionSpec as P

D_MODEL = 2048
THETA = 10000.0
EPS = 1e-06
FLOOR = -1e30
MESH = ("z3", "z2", "z1", "z0", "c", "y1", "y0", "x1", "x0")
SP, TP = MESH[:5], MESH[5:]
SP_ORDER = ("c", "z1", "z0", "z3", "z2")
TP_ORDER = ("y0", "x0", "y1", "x1")
N_SP = 32
N_TP = 16
TOK = 64
SLOTS = 192
F32 = jnp.float32
BF = jnp.bfloat16

ROWS = 28
LANE_POS, LANE_HI, LANE_LO, LANE_FLAG = 64, 65, 66, 67


def iota(shape, dim):
    return lax.broadcasted_iota(jnp.int32, shape, dim)


def div6(v):
    return (v * 10923) >> 16


def div3(v):
    return (v * 21846) >> 16


def div28(v):
    return (v * 2341) >> 16


def dot(a, b):
    return jnp.dot(a, b, preferred_element_type=F32)


def dot_nt(a, b):
    return lax.dot_general(a, b, (((1,), (1,)), ((), ())), preferred_element_type=F32)


def dot_tn(a, b):
    return lax.dot_general(a, b, (((0,), (0,)), ((), ())), preferred_element_type=F32)


def exact_tn(a, b):
    return lax.dot_general(
        a, b, (((0,), (0,)), ((), ())), precision=lax.Precision.HIGHEST, preferred_element_type=F32
    )


def reordered(peer, order, names):
    bits = [((peer >> (len(order) - 1 - i)) & 1) << (len(names) - 1 - names.index(axis)) for i, axis in enumerate(order)]
    return sum(bits[1:], bits[0])


def source_of(peer):
    return reordered(peer, SP_ORDER, SP)


TP_PLACES = tuple(reordered(piece, TP_ORDER, TP) for piece in range(N_TP))


def columns(piece):
    return slice(TP_PLACES[piece] * 128, (TP_PLACES[piece] + 1) * 128)


def picks(mask):
    return jnp.where(mask, 1.0, 0.0).astype(BF)


def side_value(block, lane):
    row = iota((SLOTS, 1), 0)
    return jnp.sum(jnp.where(iota(block.shape, 1) == lane + 4 * (row - 3 * div3(row)), block, 0.0), axis=1, keepdims=True)


def from_rows(source, row):
    count = source.shape[0]
    return picks(iota((count, N_SP * ROWS), 1) == source * ROWS + row)


def pack_kernel(
    tp_ref, wide_hbm, narrow_hbm, rope_hbm, lat_hbm, gain_hbm, res_hbm, ids_hbm, w_hbm, cos_ref, sin_ref, out_ref, sel_ref,
    ids_ref, w_ref, wide_ref, narrow_ref, rope_ref, lat_ref, gain_ref, res_ref, sems,
):
    t = tp_ref[0]
    own_columns = res_hbm.at[:, pl.ds(pl.multiple_of(t * 128, 128), 128)]
    sources = (ids_hbm, w_hbm, wide_hbm, narrow_hbm, rope_hbm, lat_hbm, gain_hbm, own_columns)
    targets = (ids_ref, w_ref, wide_ref, narrow_ref, rope_ref, lat_ref, gain_ref, res_ref)
    copies = [pltpu.make_async_copy(a, b, sems.at[i]) for i, (a, b) in enumerate(zip(sources, targets))]
    for copy in copies:
        copy.start()
    src, dst = iota((16, 128), 0), iota((16, 128), 1)
    turning = (dst < 32) | (dst >= 96)
    spread = jnp.where(turning & ((dst & 15) == src), 1.0, 0.0)
    cos = exact_tn(cos_ref[...], spread) + jnp.where((iota((TOK, 128), 1) >= 32) & (iota((TOK, 128), 1) < 96), 1.0, 0.0)
    sin = exact_tn(sin_ref[...], jnp.where((dst & 16) == 0, -spread, spread))
    src, dst = iota((128, 128), 0), iota((128, 128), 1)
    swap = picks(src == dst + jnp.where((dst & 16) == 0, 16, -16))
    first, after = picks(src == dst), picks(src + 32 == dst)
    twice = picks((iota((TOK, 128), 1) & 63) == iota((TOK, 128), 0))
    row = iota((4 * ROWS, 128), 0)
    peer = div28(row)
    place = row - peer * ROWS
    dest = source_of(peer)
    kind = div6(place)
    slot = dest * 6 + place - kind * 6
    lanes = iota((4 * ROWS, 128), 1)
    start = t * 2 + (place & 1)
    block = (place >> 1) - 9
    want_query = jnp.where(kind < 2, slot + kind * 1024, -100000)
    want_rest = jnp.where(kind == 2, slot, -100000)
    want_side = jnp.where(place >= 26, dest * 2 + place - 26 + 1024, -100000)
    lat_masks = [
        [picks(lanes == jnp.where((block >> 1) == pair, start + half * 32 + (block & 1) * 64, -1)) for pair in range(2)]
        for half in range(2)
    ]

    copies[0].wait()
    copies[1].wait()
    before = picks(iota((TOK, TOK), 0) < iota((TOK, TOK), 1))
    named = [jnp.where(ids_ref[k : k + 1, :] == iota((TOK, TOK), 0), 1.0, 0.0) for k in range(2)]
    rank = dot((named[0] + named[1]).astype(BF), before)
    slots = [
        ids_ref[k : k + 1, :] * 3 + jnp.sum(named[k] * rank, axis=0, keepdims=True).astype(jnp.int32) for k in range(2)
    ]

    def either(want):
        return picks((slots[0] == want) | (slots[1] == want))

    place = iota((SLOTS, TOK), 0)
    peer = div6(place)
    sel_ref[...] = either(source_of(peer) * 6 + place - peer * 6)
    lane, token = iota((TOK, 128), 1), iota((TOK, 128), 0).astype(F32)
    expert = iota((TOK, TOK), 0)
    side = 0.0
    for third in range(3):
        high, low, flag = 0.0, 0.0, 0.0
        for k in range(2):
            mask = slots[k] == expert * 3 + third
            w = w_ref[k : k + 1, :]
            w_hi = w.astype(BF).astype(F32)
            high = high + jnp.where(mask, w_hi, 0.0)
            low = low + jnp.where(mask, w - w_hi, 0.0)
            flag = flag + jnp.where(mask, 1.0 - k, 0.0)
        at = lane - 4 * third
        side = side + dot(either(expert * 3 + third), jnp.where(at == LANE_POS, token, 0.0).astype(BF))
        side = side + dot(high.astype(BF), picks(at == LANE_HI)) + dot(low.astype(BF), picks(at == LANE_LO))
        side = side + dot(flag.astype(BF), picks(at == LANE_FLAG))
    keys = [dot(slot.astype(F32).astype(BF), twice).astype(jnp.int32) for slot in slots]
    upper = iota((1, 128), 1) >= 64
    query_keys = [jnp.where(upper, key + 1024, key) for key in keys]
    rest_keys = [jnp.where(upper, -1, key) for key in keys]
    side_key = jnp.where(upper, (iota((1, 128), 1) & 63) + 1024, -1)

    for copy in copies[2:]:
        copy.wait()

    def turned(block):
        return (block.astype(F32) * cos + dot(block, swap) * sin).astype(BF)

    q_rest = turned((dot(wide_ref[:, 128:], first[:32]) + dot(narrow_ref[...], after[:96])).astype(BF))
    rope = turned(dot_tn(rope_ref[...], first[:32]).astype(BF))
    lat = lat_ref[...].astype(F32)
    scaled = lat * lax.rsqrt(jnp.mean(lat * lat, axis=1, keepdims=True) + EPS)
    normed = (scaled * gain_ref[...]).astype(BF)
    side = side + dot(picks(iota((TOK, TOK), 1) == ((expert >> 1) & 1) * 32 + t * 2 + (expert & 1)), rope)
    lat_rows = [
        jnp.concatenate([normed[:, f * 128 : (f + 1) * 128] for f in (2 * pair, 2 * pair + 1)], axis=0) for pair in range(2)
    ]
    lat_parts = [dot(masks[0], lat_rows[0]) + dot(masks[1], lat_rows[1]) for masks in lat_masks]
    query_rows = jnp.concatenate([wide_ref[:, :128], q_rest], axis=0)
    rest_rows = jnp.concatenate([res_ref[...], side.astype(BF)], axis=0)
    for part in range(N_SP // 4):
        away = source_of(4 * part)
        want = want_query + 6 * away
        out = dot(picks((query_keys[0] == want) | (query_keys[1] == want)), query_rows)
        want = want_rest + 6 * away
        mask = (rest_keys[0] == want) | (rest_keys[1] == want) | (side_key == want_side + 2 * away)
        out = out + dot(picks(mask), rest_rows)
        out_ref[part * 4 * ROWS : (part + 1) * 4 * ROWS, :] = (out + lat_parts[away & 1]).astype(BF)


def slots_kernel(arr_ref, out_ref):
    row = iota((SLOTS, 1), 0)
    source = div6(row)
    place = row - source * 6
    for i, start in enumerate((place, place + 6, place + 12, 26 + div3(place))):
        out_ref[:, i * 128 : (i + 1) * 128] = dot(from_rows(source, start), arr_ref[...]).astype(BF)


def spread_kernel(arr_ref, out_ref):
    n = iota((TOK, 1), 0)
    rows = [dot(from_rows(n >> 1, 18 + 2 * f + (n & 1)), arr_ref[...]).astype(BF) for f in range(4)]
    rope = dot(from_rows(n >> 1, 26 + (n & 1)), arr_ref[...]).astype(BF)
    packed = jnp.zeros((16, 128), F32)
    src, dst = iota((128, 128), 0), iota((128, 128), 1)
    for b in range(4):
        packed = packed + dot(rope[16 * b : 16 * (b + 1)], picks((src < 32) & (dst == src + 32 * b)))
    packed = packed.astype(BF)
    for copy in range(N_TP):
        for f in range(4):
            out_ref[copy, f * TOK : (f + 1) * TOK, :] = rows[f]
        out_ref[copy, 4 * TOK :, :] = packed


def keys_kernel(lat_ref, wide_ref, narrow_ref, out_ref):
    rows = N_TP * TOK
    wide = jnp.zeros((rows, 256), F32)
    narrow = jnp.zeros((rows, 128), F32)
    for pair in range(2):
        parts = [lat_ref[:, f * TOK : (f + 1) * TOK, :].reshape(rows, 128) for f in (2 * pair, 2 * pair + 1)]
        part = jnp.concatenate(parts, axis=1)
        wide = wide + dot(part, wide_ref[pair * 256 : (pair + 1) * 256, :])
        narrow = narrow + dot(part, narrow_ref[pair * 256 : (pair + 1) * 256, :])
    wide, narrow = wide.astype(BF), narrow.astype(BF)
    packed = lat_ref[:, 4 * TOK :, :].reshape(256, 128)
    src, dst = iota((128, 128), 0), iota((128, 128), 1)
    pieces = []
    for b in range(4):
        moved = dot(packed, picks((dst >= 96) & (src == dst - 96 + 32 * b)))
        pieces.append(moved.astype(BF).reshape(N_TP, 16, 128))
    rope = jnp.concatenate(pieces, axis=1).reshape(rows, 128)
    out_ref[0] = wide[:, :128]
    out_ref[1] = wide[:, 128:]
    shifted = dot(narrow, picks((src < 64) & (dst == src + 32)))
    out_ref[2] = (shifted + rope.astype(F32)).astype(BF)
    out_ref[3] = dot(narrow, picks((src >= 64) & (dst == src - 64))).astype(BF)


def half_attention(half, slot_ref, kv_ref):
    q = slot_ref[:, :256]
    side = slot_ref[:, 384:].astype(F32)
    row_pos = source_of(div6(iota((SLOTS, 1), 0))) * TOK + side_value(side, LANE_POS).astype(jnp.int32)
    src, dst = iota((128, 128), 0), iota((128, 128), 1)
    q_rest = q[:, 128:]
    wide_q = jnp.concatenate([q[:, :128], dot(q_rest, picks((src < 32) & (dst == src + 96))).astype(BF)], axis=1)
    narrow_q = jnp.where(iota((SLOTS, 128), 1) >= 32, q_rest.astype(F32), 0.0).astype(BF)
    n = iota((1, N_TP * TOK), 1)
    source, taken = source_of((n & 63) >> 1), reordered(n >> 6, TP_ORDER, TP)
    allowed = source * TOK + taken * 2 + (n & 1) + half * 32 <= row_pos
    wide = dot_nt(wide_q, jnp.concatenate([kv_ref[0], kv_ref[2]], axis=1))
    narrow = dot_nt(narrow_q, kv_ref[2])
    return [jnp.where(allowed, s, FLOOR) for s in (wide, narrow)]


RATES = tuple(width ** -0.5 * 1.4426950408889634 for width in (160, 96))


def weighed(scores, peak, rate, values):
    e = jnp.exp2((scores - peak) * rate)
    return jnp.sum(e, axis=1, keepdims=True), dot(e.astype(BF), values)


def attend_own_kernel(core_ref, slot_ref, kv_ref, peak_ref, total_ref, sum_ref):
    for i, scores in enumerate(half_attention(core_ref[0], slot_ref, kv_ref)):
        peak = jnp.max(scores, axis=1, keepdims=True)
        total, summed = weighed(scores, peak, RATES[i], kv_ref[1 + 2 * i])
        peak_ref[i] = jnp.broadcast_to(peak, (SLOTS, 128))
        total_ref[i] = jnp.broadcast_to(total, (SLOTS, 128))
        sum_ref[i] = summed


def attend_rest_kernel(core_ref, slot_ref, kv_ref, peak_ref, total_ref, sum_ref, wide_out_ref, narrow_out_ref, out_ref):
    attended = []
    for i, scores in enumerate(half_attention(1 - core_ref[0], slot_ref, kv_ref)):
        old = peak_ref[i][:, :1]
        peak = jnp.maximum(old, jnp.max(scores, axis=1, keepdims=True))
        total, summed = weighed(scores, peak, RATES[i], kv_ref[1 + 2 * i])
        kept = jnp.exp2((old - peak) * RATES[i])
        attended.append(((summed + kept * sum_ref[i]) / (total + kept * total_ref[i][:, :1])).astype(BF))
    wide_att, narrow_att = attended[0], attended[1][:, :64]
    for pair in range(N_TP // 2):
        ends = columns(2 * pair), columns(2 * pair + 1)
        wide, narrow = (jnp.concatenate([ref[:, c] for c in ends], axis=1) for ref in (wide_out_ref, narrow_out_ref))
        both = (dot(wide_att, wide) + dot(narrow_att, narrow)).astype(BF)
        out_ref[2 * pair] = both[:, :128]
        out_ref[2 * pair + 1] = both[:, 128:]


def stream_kernel(part_ref, slot_ref, out_ref):
    total = jnp.zeros((SLOTS, 128), F32)
    for piece in range(N_TP):
        total = total + part_ref[piece].astype(F32)
    stream = (slot_ref[:, 256:384].astype(F32) + total.astype(BF).astype(F32)).astype(BF)
    for copy in range(N_TP):
        out_ref[copy] = stream


def expert_kernel(x_ref, slot_ref, gain_ref, eg_ref, eu_ref, ed_ref, sg_ref, su_ref, sd_ref, out_ref):
    squares = jnp.zeros((SLOTS, 128), F32)
    for piece in range(N_TP):
        x = x_ref[piece].astype(F32)
        squares = squares + x * x
    scale = lax.rsqrt(jnp.sum(squares, axis=1, keepdims=True) * (1.0 / D_MODEL) + EPS)
    into = jnp.zeros((SLOTS, 384), F32)
    for pair in range(N_TP // 2):
        ends = columns(2 * pair), columns(2 * pair + 1)
        x = jnp.concatenate([x_ref[2 * pair], x_ref[2 * pair + 1]], axis=1).astype(F32)
        x = (x * scale * jnp.concatenate([gain_ref[:, c] for c in ends], axis=1)).astype(BF)
        halves = [
            jnp.concatenate([eg_ref[0, :, c], eg_ref[1, :, c], sg_ref[:, c], eu_ref[0, :, c], eu_ref[1, :, c], su_ref[:, c]], axis=0)
            for c in ends
        ]
        into = into + dot_nt(x, jnp.concatenate(halves, axis=1))
    gate, up = into[:, :192], into[:, 192:]
    hidden = (gate / (1.0 + jnp.exp(-gate))) * up
    side = slot_ref[:, 384:].astype(F32)
    weight = side_value(side, LANE_HI) + side_value(side, LANE_LO)
    flag = side_value(side, LANE_FLAG)
    owner = div3(iota((SLOTS, 128), 0)) & 1
    routed_hidden = jnp.where(owner == (iota((SLOTS, 128), 1) >> 6), hidden[:, :128], 0.0).astype(BF)
    shared_hidden = hidden[:, 128:].astype(BF)
    for pair in range(N_TP // 2):
        ends = columns(2 * pair), columns(2 * pair + 1)
        routed_down, shared_down = (jnp.concatenate([ref[:, c] for c in ends], axis=1) for ref in (ed_ref, sd_ref))
        both = (weight * dot(routed_hidden, routed_down) + flag * dot(shared_hidden, shared_down)).astype(BF)
        out_ref[2 * pair] = both[:, :128]
        out_ref[2 * pair + 1] = both[:, 128:]


def give_back_kernel(part_ref, stream_ref, slot_ref, out_ref):
    total = jnp.zeros((SLOTS, 128), F32)
    for piece in range(N_TP):
        total = total + part_ref[piece].astype(F32)
    flag = side_value(slot_ref[:, 384:].astype(F32), LANE_FLAG)
    out_ref[...] = (total + flag * stream_ref[0].astype(F32)).astype(BF)


def finish_kernel(sel_ref, back_ref, out_ref):
    out_ref[...] = dot_tn(sel_ref[...], back_ref[...]).astype(BF)


VMEM = pl.BlockSpec(memory_space=pltpu.VMEM)
SMEM = pl.BlockSpec(memory_space=pltpu.SMEM)


HBM = pl.BlockSpec(memory_space=pltpu.HBM)


def run(kernel, outs, *args, scalars=0, plain=0, spread=True, kind=BF, scratch=()):
    spaces = [pltpu.HBM if i < plain else pltpu.VMEM for i in range(scalars, len(args))]
    placed = [pltpu.with_memory_space_constraint(a, m) for a, m in zip(args[scalars:], spaces)]
    args = [*args[:scalars], *placed]
    return pl.pallas_call(
        kernel,
        out_shape=[pltpu.VMEM(shape, kind) for shape in outs] if spread else jax.ShapeDtypeStruct(outs[0], BF),
        in_specs=[SMEM] * scalars + [HBM if m is pltpu.HBM else VMEM for m in spaces],
        out_specs=[VMEM] * len(outs) if spread else VMEM,
        scratch_shapes=scratch,
        compiler_params=pltpu.CompilerParams(vmem_limit_bytes=24 << 20),
        name=kernel.__name__,
    )(*args)


def swap_all(values, axes):
    return lax.all_to_all(values, axes, split_axis=0, concat_axis=0, tiled=True)


def local(
    wide_queries,
    narrow_queries,
    kv_latent,
    rope_key,
    latent_gain,
    wide_kv_weight,
    narrow_kv_weight,
    wide_out_weight,
    narrow_out_weight,
    residual,
    norm_gain,
    route_ids,
    route_weights,
    expert_gate,
    expert_up,
    expert_down,
    shared_gate,
    shared_up,
    shared_down,
):
    t = lax.axis_index(TP).astype(jnp.int32)[None]
    core = lax.axis_index("c").astype(jnp.int32)[None]
    frequency = THETA ** (-2.0 * jnp.arange(16, dtype=F32) / 32)
    positions = lax.axis_index(SP) * TOK + jnp.arange(TOK, dtype=jnp.int32)
    angles = frequency[:, None] * positions.astype(F32)[None, :]
    payload, chosen = run(
        pack_kernel, [(N_SP * ROWS, 128), (SLOTS, TOK)],
        t, wide_queries, narrow_queries, rope_key.T, kv_latent, latent_gain[None, :], residual,
        route_ids.T, route_weights.T, jnp.cos(angles), jnp.sin(angles),
        scalars=1,
        plain=9,
        scratch=[
            pltpu.VMEM((2, TOK), jnp.int32),
            pltpu.VMEM((2, TOK), F32),
            pltpu.VMEM((TOK, 160), BF),
            pltpu.VMEM((TOK, 96), BF),
            pltpu.VMEM((32, TOK), BF),
            pltpu.VMEM((TOK, 512), BF),
            pltpu.VMEM((1, 512), F32),
            pltpu.VMEM((TOK, 128), BF),
            pltpu.SemaphoreType.DMA((8,)),
        ],
    )
    arrived = swap_all(payload.reshape(N_SP, ROWS // 2, 2, 128), SP_ORDER).reshape(N_SP * ROWS, 128)
    (spread,) = run(spread_kernel, [(N_TP, 272, 128)], arrived)
    latents = swap_all(spread, TP_ORDER)
    (slots,) = run(slots_kernel, [(SLOTS, 512)], arrived)
    (own,) = run(keys_kernel, [(4, N_TP * TOK, 128)], latents, wide_kv_weight, narrow_kv_weight)
    other = lax.ppermute(own, "c", [(0, 1), (1, 0)])
    state = run(attend_own_kernel, [(2, SLOTS, 128)] * 3, core, slots, own, scalars=1, kind=F32)
    (partial,) = run(
        attend_rest_kernel, [(N_TP, SLOTS, 128)],
        core, slots, other, *state, wide_out_weight, narrow_out_weight,
        scalars=1,
    )
    (copies,) = run(stream_kernel, [(N_TP, SLOTS, 128)], swap_all(partial, TP_ORDER), slots)
    rows = swap_all(copies, TP_ORDER)
    (partial,) = run(
        expert_kernel, [(N_TP, SLOTS, 128)],
        rows, slots, norm_gain[None, :],
        expert_gate.swapaxes(1, 2), expert_up.swapaxes(1, 2), expert_down.reshape(128, D_MODEL),
        shared_gate.T, shared_up.T, shared_down,
    )
    (back,) = run(give_back_kernel, [(SLOTS, 128)], swap_all(partial, TP_ORDER), copies, slots)
    back = swap_all(back.reshape(N_SP, 3, 2, 128), SP_ORDER).reshape(SLOTS, 128)
    return run(finish_kernel, [(TOK, 128)], chosen, back, spread=False)


def solution(mesh):
    torus = Mesh(mesh.devices.reshape((2,) * len(MESH)), MESH)
    return jax.shard_map(
        local,
        mesh=torus,
        in_specs=(
            P(SP, TP),
            P(SP, TP),
            P(SP, None),
            P(SP, None),
            P(),
            P(None, TP),
            P(None, TP),
            P(TP, None),
            P(TP, None),
            P(SP, None),
            P(),
            P(SP, None),
            P(SP, None),
            P(SP, None, TP),
            P(SP, None, TP),
            P(SP, TP, None),
            P(None, TP),
            P(None, TP),
            P(TP, None),
        ),
        out_specs=P(SP, TP),
        check_vma=False,
    )
```
